256 devices in a mesh: grp: 2 (over y), sp: 32 (over z, core), tp: 4 (over x).
Axes of the slice: x: 4, y: 2, z: 16, core: 2. Of those that a mesh axis runs over, the one named last changes fastest.
The devices are a block of a 4x16x16 slice.
Arguments:
- query_rows: bfloat16 [32768, 512], P(('grp', 'sp'), 'tp'), parts along dimension 0, may hold values from -12 to 12
- key_rows: bfloat16 [32768, 512], P(('grp', 'sp'), 'tp'), parts along dimension 0, may hold values from -12 to 12
- value_rows: bfloat16 [32768, 512], P(('grp', 'sp'), 'tp'), parts along dimension 0, may hold values from -12 to 12
- residual: bfloat16 [32768, 2048], P(('grp', 'sp', 'tp')), parts along dimension 0, may hold values from -6 to 6
- output_weight: bfloat16 [512, 2048], P('tp'), may hold values from -0.25 to 0.25
- first_gain: float32 [2048], replicated, may hold values from 0.1 to 1.9
- first_bias: float32 [2048], replicated, may hold values from -3 to 3
- expert_ids: int32 [32768, 4], P(('grp', 'sp', 'tp')), parts along dimension 0, may hold values from 0 to 127, all different within a row; in each aligned block of 128 rows (0 to 127, 128 to 255, ...) at most 6 rows name the same one
- expert_share: float32 [32768, 4], P(('grp', 'sp', 'tp')), parts along dimension 0, may hold values from 0.3 to 1.2
- gate_weight: bfloat16 [128, 2048, 256], P(('sp', 'tp')), may hold values from -0.125 to 0.125
- up_weight: bfloat16 [128, 2048, 256], P(('sp', 'tp')), may hold values from -0.125 to 0.125
- down_weight: bfloat16 [128, 256, 2048], P(('sp', 'tp')), may hold values from -0.375 to 0.375
- shared_gate: bfloat16 [2048, 512], replicated, may hold values from -0.125 to 0.125
- shared_up: bfloat16 [2048, 512], replicated, may hold values from -0.125 to 0.125
- shared_down: bfloat16 [512, 2048], replicated, may hold values from -0.25 to 0.25
- second_gain: float32 [2048], replicated, may hold values from 0.1 to 1.9
- second_bias: float32 [2048], replicated, may hold values from -3 to 3
Outputs:
- layer_out: bfloat16 [32768, 2048], P(('grp', 'sp', 'tp')), parts along dimension 0
The draws below stay inside these ranges and needn't reach their ends.
There are 2 independent parts, one for each index of `grp`. The reference program is written for one: setup_inputs(seed, part) draws one part's arguments, and reference() takes and returns one part's arrays. A program takes and returns all parts, laid end to end along the dimension named above; an argument that names none is the same for every part. Nothing has to cross between parts.
Inputs may be any that keep to these rules, and one draw needn't show every extreme that they name: `expert_ids`: each row names 4 different experts. Among the rows of one device (aligned blocks of 128 rows) no expert is named by more than 6 rows, a bound that some block reaches.
All inputs are finite; a program needn't handle non-finite values.
Results may differ from the reference program's by a relative error of at most 0.012.
Values may be sent and summed in bfloat16 or wider, within the bound.
A program may use at most 128 MiB of HBM per device.

```python
import math
import jax
import jax.numpy as jnp
import numpy as np
from jax import lax

HEADS = 4
HEAD_DIM = 128
D = 2048
EFF = 256
SFF = 512
TOP_K = 4
KBLK = 128
T_SP = 512
TOK = 128
SEQUENCE_LENGTH = 16384
QH = 512
EXPERTS = 128
CAP = 6


def head_plan(key):
    baseline_value = jax.random.fold_in(key, 101)
    direction_key, selection_key, quick_rate_key, gentle_rate_key, multiplier_key, spike_event_key = jax.random.split(baseline_value, 6)
    directions = jax.random.normal(direction_key, (HEADS, HEAD_DIM), jnp.float32)
    directions = directions / jnp.sqrt(jnp.sum(directions * directions, axis=1, keepdims=True))
    slow_share = 0.5
    is_slow = jax.random.uniform(selection_key, (HEADS,), jnp.float32) < slow_share
    fast_rate = jax.random.uniform(quick_rate_key, (HEADS,), jnp.float32, 2.5, 3.8)
    slow_rate = math.log(SEQUENCE_LENGTH) + 1.0 + jax.random.uniform(gentle_rate_key, (HEADS,), jnp.float32, 0.0, 0.4)
    rates = jnp.where(is_slow, slow_rate, fast_rate)
    factors = jnp.exp(jax.random.uniform(multiplier_key, (SEQUENCE_LENGTH // KBLK, HEADS), jnp.float32, -0.15, 0.15))
    position_indices = jnp.arange(SEQUENCE_LENGTH)
    coefs = factors[position_indices // KBLK]
    spike_events = jax.random.randint(spike_event_key, (3,), 0, SEQUENCE_LENGTH)
    spike_hits = jnp.any(position_indices[:, None] == spike_events[None, :], axis=1)
    coefs = jnp.where(spike_hits[:, None], 1.2 / rates[None, :], coefs)
    return (directions, rates, coefs)


def noise_for(key):
    noise = 0.5 * jax.random.normal(key, (SEQUENCE_LENGTH, HEADS, HEAD_DIM), jnp.float32)
    return noise


def draw_query_rows(key, part):
    directions, rates, coefs = head_plan(key)
    amps = jnp.sqrt(rates) * HEAD_DIM ** 0.25
    noise = noise_for(jax.random.fold_in(key, 211))
    rows = noise - amps[None, :, None] * directions[None, :, :]
    return jnp.clip(rows.reshape(SEQUENCE_LENGTH, QH), -12.0, 12.0).astype(jnp.bfloat16)


def draw_key_rows(key, part):
    directions, rates, coefs = head_plan(key)
    amps = jnp.sqrt(rates) * HEAD_DIM ** 0.25
    noise = noise_for(jax.random.fold_in(key, 223))
    rows = noise + (coefs * amps[None, :])[:, :, None] * directions[None, :, :]
    return jnp.clip(rows.reshape(SEQUENCE_LENGTH, QH), -12.0, 12.0).astype(jnp.bfloat16)


def draw_value_rows(key, part):
    key_noise = jax.random.fold_in(key, 227)
    key_offset = jax.random.fold_in(key, 229)
    noise = jax.random.normal(key_noise, (SEQUENCE_LENGTH, HEADS, HEAD_DIM), jnp.float32)
    offsets = jax.random.normal(key_offset, (16, HEADS, HEAD_DIM), jnp.float32)
    region = jnp.arange(SEQUENCE_LENGTH) * 16 // SEQUENCE_LENGTH
    rows = noise + offsets[region]
    return jnp.clip(rows.reshape(SEQUENCE_LENGTH, QH), -12.0, 12.0).astype(jnp.bfloat16)


def block_levels(own_key, shape, cuts, low, largest):
    def one(dim, blocks):
        draws = jax.random.uniform(jax.random.fold_in(jax.random.fold_in(own_key, 6), dim), (blocks,), jnp.float32, low / len(cuts), largest / len(cuts))
        return jnp.repeat(jnp.exp(draws), shape[dim] // blocks).reshape((-1,) + (1,) * (len(shape) - dim - 1))

    level = one(*cuts[0])
    for cut in cuts[1:]:
        level = level * one(*cut)
    return level


def routed_block(own_key, own, number, rows, amount, top, most, skew):
    order = jax.random.permutation(own_key, amount)
    crowded, usual = load_shares(amount, rows * top, most, skew, True), load_shares(amount, rows * top, most, skew, False)
    places = jnp.arange(amount)

    def named(sizes, rotation):
        used = int((sizes > 0).sum())
        fixed = max(1, used // 4)
        moved = fixed + (places - fixed + rotation * (used - fixed)) % max(1, amount - fixed)
        return jnp.zeros((amount,), jnp.int32).at[order[jnp.where(places < fixed, places, moved)]].set(jnp.asarray(sizes, jnp.int32))

    sizes = jnp.where(number % 4 == 0, named(crowded, number // 4), named(usual, number - number // 4 - 1))
    mixed = jax.random.permutation(jax.random.fold_in(own, 3), amount)
    source_of, taker = mixed[0:amount // 2 * 2:2], mixed[1:amount // 2 * 2:2]
    slack = jnp.minimum(sizes[source_of] - 1, most - sizes[taker]) // 2
    slack = jnp.where((source_of == order[0]) | (taker == order[0]) | (sizes[taker] == 0), 0, jnp.maximum(slack, 0))
    moved = jax.random.randint(jax.random.fold_in(own, 4), (amount // 2,), 0, 1 << 20) % (slack + 1)
    sizes = sizes.at[source_of].add(-moved).at[taker].add(moved)
    items = jnp.searchsorted(jnp.cumsum(sizes), jnp.arange(rows * top), side="right").astype(jnp.int32)
    listing = items.reshape(top, rows).T
    listing = listing[jax.random.permutation(jax.random.fold_in(own, 1), rows)]
    rotation = jax.random.randint(jax.random.fold_in(own, 2), (rows, 1), 0, top)
    return jnp.take_along_axis(listing, (jnp.arange(top)[None, :] + rotation) % top, axis=1)


def load_shares(number_of, total, reach, slope, full):
    loads = [(1 << 20) // math.isqrt(grade ** slope) + 1 for grade in range(1, number_of + 1)]
    largest = reach if full else min(reach, max(-(-total // number_of), total * loads[0] // sum(loads)))
    least = 1 if total - largest >= number_of - 1 else 0
    holding, rest = [largest] + [least] * (number_of - 1), total - largest - least * (number_of - 1)
    while rest > 0:
        candidates = [i for i in range(1, number_of) if holding[i] < largest] or [i for i in range(1, number_of) if holding[i] < reach]
        pool, budget = sum([loads[i] for i in candidates]), rest
        for i in candidates:
            extra = min(reach - holding[i], max(1, budget * loads[i] // pool), rest)
            holding[i] = holding[i] + extra
            rest = rest - extra
    return np.array(holding)


def normal_values(rng, shape, deviation, limit, cuts=(), kind=jnp.bfloat16):
    values = jax.random.normal(rng, shape, jnp.float32) * deviation
    if len(cuts) > 0:
        values = block_levels(rng, shape, cuts, -0.22, 0.18) * values
    return jnp.clip(values, min=-limit, max=limit).astype(kind)


def setup_inputs(seed: int = 0, part: int = 0) -> dict:
    splits = jax.random.split(jax.random.key(seed), 18)
    part_keys = jax.random.split(jax.random.fold_in(splits[17], part), 18)
    query_rows = draw_query_rows(jax.random.fold_in(jax.random.fold_in(splits[17], part), 71), part)
    key_rows = draw_key_rows(jax.random.fold_in(jax.random.fold_in(splits[17], part), 71), part)
    value_rows = draw_value_rows(jax.random.fold_in(jax.random.fold_in(splits[17], part), 71), part)
    residual = normal_values(part_keys[3], (SEQUENCE_LENGTH, D), 1.0, 6.0, ((0, 128),))
    output_weight = normal_values(splits[4], (QH, D), QH ** -0.5, 0.25, ((0, 4),))
    first_gain = jnp.clip(1.0 + 0.18 * jax.random.normal(splits[5], (D,), jnp.float32), 0.1, 1.9)
    first_bias = normal_values(splits[6], (D,), 0.5, 3.0, (), jnp.float32)
    expert_ids_keys = jax.random.split(jax.random.fold_in(part_keys[7], 1), SEQUENCE_LENGTH // TOK)
    expert_ids_turns = jax.random.permutation(jax.random.fold_in(part_keys[7], 3), SEQUENCE_LENGTH // TOK)
    expert_ids = jax.vmap(lambda own, number: routed_block(jax.random.fold_in(part_keys[7], 2), own, number, TOK, EXPERTS, TOP_K, CAP, 1))(expert_ids_keys, expert_ids_turns).reshape((SEQUENCE_LENGTH, TOP_K))
    expert_share = jnp.clip(jnp.exp(math.log(1.2) - 1.3862944 * jax.random.uniform(part_keys[8], (SEQUENCE_LENGTH, TOP_K), jnp.float32) ** block_levels(part_keys[8], (SEQUENCE_LENGTH, TOP_K), ((0, 128),), -0.2, 0.2)), 0.3, 1.2)
    gate_weight = normal_values(splits[9], (EXPERTS, D, EFF), D ** -0.5, 0.125, ((0, 128),))
    up_weight = normal_values(splits[10], (EXPERTS, D, EFF), D ** -0.5, 0.125, ((0, 128),))
    down_weight = normal_values(splits[11], (EXPERTS, EFF, D), EFF ** -0.5, 0.375, ((0, 128),))
    shared_gate = normal_values(splits[12], (D, SFF), D ** -0.5, 0.125)
    shared_up = normal_values(splits[13], (D, SFF), D ** -0.5, 0.125)
    shared_down = normal_values(splits[14], (SFF, D), SFF ** -0.5, 0.25)
    second_gain = jnp.clip(1.0 + 0.18 * jax.random.normal(splits[15], (D,), jnp.float32), 0.1, 1.9)
    second_bias = normal_values(splits[16], (D,), 0.5, 3.0, (), jnp.float32)
    return {"query_rows": query_rows, "key_rows": key_rows, "value_rows": value_rows, "residual": residual, "output_weight": output_weight, "first_gain": first_gain, "first_bias": first_bias, "expert_ids": expert_ids, "expert_share": expert_share, "gate_weight": gate_weight, "up_weight": up_weight, "down_weight": down_weight, "shared_gate": shared_gate, "shared_up": shared_up, "shared_down": shared_down, "second_gain": second_gain, "second_bias": second_bias}


NORM_EPS = 1e-05

def layer_norm(summed, gains, offset):
    average = lax.optimization_barrier(jnp.mean(summed, axis=-1, keepdims=True))
    centred = summed - average
    spread = lax.optimization_barrier(jnp.mean(centred * centred, axis=-1, keepdims=True))
    return centred * lax.rsqrt(spread + NORM_EPS) * gains.astype(jnp.float32) + offset.astype(jnp.float32)

def stick_attention(query_rows, key_rows, value_rows):
    scale = HEAD_DIM ** (-0.5)
    queries = query_rows.astype(jnp.float32).reshape(SEQUENCE_LENGTH // T_SP, T_SP, HEADS, HEAD_DIM)
    keys = key_rows.astype(jnp.float32).reshape(SEQUENCE_LENGTH // KBLK, KBLK, HEADS, HEAD_DIM)
    values = value_rows.astype(jnp.float32).reshape(SEQUENCE_LENGTH // KBLK, KBLK, HEADS, HEAD_DIM)

    def one_block(packed):
        query_block, which = packed
        query_pos = which * T_SP + jnp.arange(T_SP, dtype=jnp.int32)
        visits = (which + 1) * (T_SP // KBLK)

        def visit(visit_no, carry):
            summed, behind = carry
            chosen = visits - 1 - visit_no
            key_block = lax.dynamic_index_in_dim(keys, chosen, 0, keepdims=False)
            value_block = lax.dynamic_index_in_dim(values, chosen, 0, keepdims=False)
            key_pos = chosen * KBLK + jnp.arange(KBLK, dtype=jnp.int32)
            score = jnp.einsum('qhd,khd->qhk', query_block, key_block) * scale
            usable = key_pos[None, None, :] < query_pos[:, None, None]
            spent = jnp.where(usable, jax.nn.softplus(score), 0.0)
            running = jnp.cumsum(spent, axis=-1)
            totals = running[..., -1]
            inside = totals[..., None] - running + spent
            weight = jnp.where(usable, jnp.exp(score - inside), 0.0)
            weight = lax.optimization_barrier(weight.astype(jnp.bfloat16)).astype(jnp.float32)
            pieces = jnp.einsum('qhk,khd->qhd', weight, value_block)
            summed = summed + pieces * jnp.exp(-behind)[..., None]
            return (summed, behind + totals)
        initial = (jnp.zeros((T_SP, HEADS, HEAD_DIM), jnp.float32), jnp.zeros((T_SP, HEADS), jnp.float32))
        summed, _ = lax.fori_loop(0, visits, visit, initial)
        return summed.reshape(T_SP, QH).astype(jnp.bfloat16)
    blocks = lax.map(one_block, (queries, jnp.arange(SEQUENCE_LENGTH // T_SP, dtype=jnp.int32)))
    return blocks.reshape(SEQUENCE_LENGTH, QH)

def expert_rows(slot_rows, gate_mat, up_mat, down_mat):
    gate_act = jnp.dot(slot_rows, gate_mat, preferred_element_type=jnp.float32)
    up_act = jnp.dot(slot_rows, up_mat, preferred_element_type=jnp.float32)
    hidden = (jax.nn.silu(gate_act) * up_act).astype(jnp.bfloat16)
    return jnp.dot(hidden, down_mat, preferred_element_type=jnp.float32).astype(jnp.bfloat16)

def reference(query_rows, key_rows, value_rows, residual, output_weight, first_gain, first_bias, expert_ids, expert_share, gate_weight, up_weight, down_weight, shared_gate, shared_up, shared_down, second_gain, second_bias):
    attended = stick_attention(query_rows, key_rows, value_rows)
    mixed = jnp.dot(attended, output_weight, preferred_element_type=jnp.float32)
    normed = layer_norm(residual.astype(jnp.float32) + mixed, first_gain, first_bias).astype(jnp.bfloat16)
    sources = SEQUENCE_LENGTH // TOK
    pair_count = TOK * TOP_K
    id_table = expert_ids.reshape(sources, pair_count).astype(jnp.int32)
    one_hot = (id_table[:, :, None] == jnp.arange(EXPERTS, dtype=jnp.int32)[None, None, :]).astype(jnp.int32)
    before = jnp.cumsum(one_hot, axis=1) - one_hot
    ranked = lax.optimization_barrier(jnp.sum(before * one_hot, axis=2)).astype(jnp.int32)
    source_ids = jnp.arange(sources, dtype=jnp.int32)[:, None]
    row_ids = (source_ids * pair_count + jnp.arange(pair_count, dtype=jnp.int32)[None, :]).astype(jnp.int32)
    columns = (source_ids * CAP + ranked).astype(jnp.int32)
    slot_table = jnp.full((EXPERTS, sources * CAP), SEQUENCE_LENGTH * TOP_K, jnp.int32).at[id_table, columns].set(row_ids)
    padded_rows = jnp.concatenate([normed, jnp.zeros((1, D), jnp.bfloat16)], axis=0)
    padded_share = jnp.concatenate([expert_share.reshape(-1).astype(jnp.float32), jnp.zeros((1,), jnp.float32)])

    def per_expert(carry, expert):
        slot_rows = slot_table[expert]
        token_of = (slot_rows // TOP_K).astype(jnp.int32)
        outputs = expert_rows(padded_rows[token_of], gate_weight[expert], up_weight[expert], down_weight[expert])
        shares = padded_share[slot_rows]
        carry = carry.at[token_of].add(outputs.astype(jnp.float32) * shares[:, None])
        return (carry, None)
    routed, _ = lax.scan(per_expert, jnp.zeros((SEQUENCE_LENGTH + 1, D), jnp.float32), jnp.arange(EXPERTS, dtype=jnp.int32))
    routed = routed[:SEQUENCE_LENGTH]
    gate_act = jnp.dot(normed, shared_gate, preferred_element_type=jnp.float32)
    up_act = jnp.dot(normed, shared_up, preferred_element_type=jnp.float32)
    shared_hidden = (jax.nn.silu(gate_act) * up_act).astype(jnp.bfloat16)
    shared_out = jnp.dot(shared_hidden, shared_down, preferred_element_type=jnp.float32)
    final = layer_norm(normed.astype(jnp.float32) + routed + shared_out, second_gain, second_bias)
    return final.astype(jnp.bfloat16)
```

```python
import functools

import jax
import jax.numpy as jnp
from jax import lax
from jax.experimental import pallas as pl
from jax.experimental.pallas import tpu as pltpu
from jax.sharding import PartitionSpec as P

HEAD_DIM = 128
KBLK = 128
NORM_EPS = 1e-05
LOG2E = 1.4426950408889634
MESH = pl.DeviceIdType.MESH
SLOTS = 8
BF16 = jnp.bfloat16
F32 = jnp.float32


def at_sp(sp):
    return {"sp": sp}


def place():
    sp = lax.axis_index("sp")
    return sp, sp // 2, sp % 2, lax.axis_index("tp")


def greet(devices):
    barrier = pltpu.get_barrier_semaphore()
    for device in devices:
        pl.semaphore_signal(barrier, inc=1, device_id=device, device_id_type=MESH)
    pl.semaphore_wait(barrier, len(devices))


def remote(src, dst, send_sem, recv_sem, device):
    return pltpu.make_async_remote_copy(
        src_ref=src,
        dst_ref=dst,
        send_sem=send_sem,
        recv_sem=recv_sem,
        device_id=device,
        device_id_type=MESH,
    )


def attention_kernel(
    nz,
    nx,
    q_ref,
    k_ref,
    v_ref,
    wo_ref,
    aux_ref,
    out_ref,
    wo_out,
    aux_out,
    kv,
    acc,
    behind,
    far,
    ring_send,
    ring_recv,
    pair_send,
    pair_recv,
    own_send,
    own_recv,
    aux_send,
    aux_recv,
    wo_send,
    wo_recv,
):
    sp, z, core, x = place()
    rows = q_ref.shape[0]
    half = rows // 2
    nsp = 2 * nz
    far_hop = nz // 2 - 1
    hop_to = (
        at_sp(lax.rem(sp + 2, nsp)),
        at_sp(lax.rem(sp + nsp - 2, nsp)),
    )
    partner = at_sp(sp + 1 - 2 * core)
    across = [{"tp": lax.rem(x + o, nx)} for o in range(1, nx)]
    greet([hop_to[0], hop_to[1], partner] + across)

    wo_rows = wo_ref.shape[0]

    def source(way, s):
        return lax.rem(z + nz - (s + 1), nz) if way == 0 else lax.rem(z + s + 1, nz)

    def piece(block, c):
        return kv.at[c // 2, block, pl.ds((c % 2) * half, half)]

    def own_piece(c):
        return (k_ref, v_ref)[c // 2].at[pl.ds((c % 2) * half, half)]

    def ring(way, s, c, block, src=None):
        return remote(
            piece(block, c) if src is None else src,
            piece(block, c),
            ring_send.at[way, s, c],
            ring_recv.at[way, s, c],
            hop_to[way],
        )

    def pair(way, s, c, block):
        return remote(
            piece(block, c),
            piece(block, c),
            pair_send.at[way, s, c],
            pair_recv.at[way, s, c],
            partner,
        )

    def own_pair(c, block):
        return remote(own_piece(c), piece(block, c), own_send.at[c], own_recv.at[c], partner)

    def aux_hop(way, s, block, src=None):
        return remote(
            aux_out.at[block] if src is None else src,
            aux_out.at[block],
            aux_send.at[way, s],
            aux_recv.at[way, s],
            hop_to[way],
        )

    def wo_copy(o, at):
        return remote(
            wo_ref,
            wo_out.at[pl.ds(at * wo_rows, wo_rows)],
            wo_send.at[o - 1],
            wo_recv.at[o - 1],
            across[o - 1],
        )

    for way in (0, 1):
        aux_hop(way, 0, z, aux_ref).start()
    for c in range(4):
        for way in (0, 1):
            ring(way, 0, c, sp, own_piece(c)).start()
        own_pair(c, sp).start()
    for o in range(1, nx):
        wo_copy(o, x).start()

    kv[0, sp] = k_ref[...]
    kv[1, sp] = v_ref[...]
    aux_out[z] = aux_ref[...]
    wo_out[pl.ds(x * wo_rows, wo_rows), :] = wo_ref[...]
    acc[...] = jnp.zeros_like(acc)
    behind[...] = jnp.zeros_like(behind)
    far[...] = jnp.zeros_like(far)

    tile = min(256, rows)
    above = lax.broadcasted_iota(jnp.int32, (KBLK, 2 * KBLK), 0)
    below = lax.broadcasted_iota(jnp.int32, (KBLK, 2 * KBLK), 1)
    sums = ((above > below) | (below >= KBLK)).astype(F32).astype(BF16)
    to_log2 = HEAD_DIM ** (-0.5) * LOG2E

    def visit(block, mode):
        @pl.loop(0, rows // tile)
        def _(t):
            here = pl.ds(pl.multiple_of(t * tile, tile), tile)
            q = q_ref[here, :]
            spent_after = (
                jnp.zeros((tile, KBLK), F32) if mode == "far" else behind[here, :]
            )
            total = jnp.zeros((tile, HEAD_DIM), F32)
            for b in reversed(range(rows // KBLK)):
                span = pl.ds(b * KBLK, KBLK)
                score = (
                    lax.dot_general(
                        q,
                        kv[0, block, span, :],
                        (((1,), (1,)), ((), ())),
                        preferred_element_type=F32,
                    )
                    * to_log2
                )
                soft = jnp.maximum(
                    score, jnp.log(1.0 + jnp.exp2(jnp.minimum(score, 64.0))) * LOG2E
                )
                if mode == "diagonal":
                    key_pos = b * KBLK + lax.broadcasted_iota(jnp.int32, (tile, KBLK), 1)
                    query_pos = t * tile + lax.broadcasted_iota(jnp.int32, (tile, KBLK), 0)
                    usable = key_pos < query_pos
                    spent = jnp.where(usable, soft, 0.0)
                else:
                    spent = soft
                added = jnp.dot(spent.astype(BF16), sums, preferred_element_type=F32)
                weight = jnp.exp2(((score - soft) - added[:, :KBLK]) - spent_after)
                if mode == "diagonal":
                    weight = jnp.where(usable, weight, 0.0)
                spent_after = spent_after + added[:, KBLK:]
                total = total + jnp.dot(
                    weight.astype(BF16), kv[1, block, span, :], preferred_element_type=F32
                )
            if mode == "far":
                far[here, :] = far[here, :] * jnp.exp2(-spent_after) + total
            else:
                acc[here, :] = acc[here, :] + total
                behind[here, :] = spent_after

    def work(s, c):
        near_chip = z - (s + 1)
        far_chip = z + s + 1 - nz
        if c < 2:

            @pl.when(near_chip >= 0)
            def _():
                visit(jnp.maximum(2 * near_chip + 1 - c, 0), "near")

        else:

            @pl.when(far_chip >= 0)
            def _():
                visit(jnp.maximum(2 * far_chip + c - 2, 0), "far")

    visit(sp, "diagonal")
    other = sp + 1 - 2 * core
    for c in range(4):
        own_pair(c, other).wait_recv()

    @pl.when(core == 1)
    def _():
        visit(other, "near")

    def of_pair(way, s):
        return 2 * source(way, s) + 1 - core

    @pl.loop(0, far_hop)
    def _(s):
        for way in (0, 1):
            aux_hop(way, s, source(way, s)).wait_recv()

            @pl.when((s < far_hop - 1) | (way == 0))
            def _():
                aux_hop(way, s + 1, source(way, s)).start()

        for c in range(4):
            for way in (0, 1):
                block = 2 * source(way, s) + core
                ring(way, s, c, block).wait_recv()
                if (c < 2) == (way == 0):
                    ring(way, s + 1, c, block).start()
                else:

                    @pl.when(s < far_hop - 1)
                    def _():
                        ring(way, s + 1, c, block).start()

                pair(way, s, c, block).start()

            @pl.when(s > 0)
            def _():
                if c == 0:
                    for way in (0, 1):
                        for c2 in range(4):
                            pair(way, s - 1, c2, of_pair(way, s - 1)).wait_recv()
                work(s - 1, c)

    last = far_hop - 1
    for way in (0, 1):
        for c2 in range(4):
            pair(way, last, c2, of_pair(way, last)).wait_recv()
    for c in range(4):
        work(last, c)
    aux_hop(0, far_hop, source(0, far_hop)).wait_recv()
    for c in range(4):
        way = c // 2
        block = 2 * source(way, far_hop) + core
        ring(way, far_hop, c, block).wait_recv()
        pair(way, far_hop, c, block).start()
    for c in range(4):
        way = c // 2
        pair(way, far_hop, c, of_pair(way, far_hop)).wait_recv()
    for c in range(2):
        work(far_hop, c)
    out_ref[...] = (acc[...] + far[...] * jnp.exp2(-behind[...])).astype(out_ref.dtype)

    for o in range(1, nx):
        wo_copy(o, lax.rem(x + nx - o, nx)).wait_recv()
        wo_copy(o, x).wait_send()
    for c in range(4):
        own_pair(c, sp).wait_send()

    @pl.loop(0, far_hop)
    def _(s):
        for way in (0, 1):
            aux_hop(way, s, z).wait_send()
            for c in range(4):
                ring(way, s, c, sp).wait_send()
                pair(way, s, c, sp).wait_send()

    aux_hop(0, far_hop, z).wait_send()
    for c in range(4):
        ring(c // 2, far_hop, c, sp).wait_send()
        pair(c // 2, far_hop, c, sp).wait_send()


def attention(nz, nx, q, k, v, wo, aux):
    rows, width = q.shape
    whole = pl.BlockSpec(memory_space=pltpu.VMEM)
    hops = nz // 2
    dma = pltpu.SemaphoreType.DMA
    flops = 6 * rows * rows * width * nz * 2
    return pl.pallas_call(
        functools.partial(attention_kernel, nz, nx),
        name="attention",
        out_shape=(
            jax.ShapeDtypeStruct((rows, width), BF16),
            jax.ShapeDtypeStruct((nx * wo.shape[0], wo.shape[1]), BF16),
            jax.ShapeDtypeStruct((nz, *aux.shape), F32),
        ),
        in_specs=[whole] * 5,
        out_specs=(whole, whole, whole),
        scratch_shapes=[
            pltpu.VMEM((2, 2 * nz, rows, width), BF16),
            pltpu.VMEM((rows, width), F32),
            pltpu.VMEM((rows, KBLK), F32),
            pltpu.VMEM((rows, width), F32),
            dma((2, hops, 4)),
            dma((2, hops, 4)),
            dma((2, hops, 4)),
            dma((2, hops, 4)),
            dma((4,)),
            dma((4,)),
            dma((2, hops)),
            dma((2, hops)),
            dma((nx - 1,)),
            dma((nx - 1,)),
        ],
        compiler_params=pltpu.CompilerParams(collective_id=0, has_side_effects=True),
        cost_estimate=pl.CostEstimate(flops=flops, bytes_accessed=1 << 20, transcendentals=0),
    )(q, k, v, wo, aux)


def slot_codes(aux, z, experts):
    width = aux.shape[1]
    picks = aux.shape[0] // 2
    number = (z * experts + lax.broadcasted_iota(jnp.int32, (experts, width), 0)).astype(F32)
    named = jnp.zeros((experts, width), F32)
    share = jnp.zeros((experts, width), F32)
    for k in range(picks):
        hit = aux[k : k + 1, :] == number
        named = named + jnp.where(hit, 1.0, 0.0)
        share = share + jnp.where(hit, aux[picks + k : picks + k + 1, :], 0.0)
    earlier = lax.broadcasted_iota(jnp.int32, (width, width), 0)
    later = lax.broadcasted_iota(jnp.int32, (width, width), 1)
    before = (earlier < later).astype(F32).astype(BF16)
    rank = jnp.dot(named.astype(BF16), before, preferred_element_type=F32)
    return jnp.where(named > 0.0, rank, -1000.0), share


def slot_matches(code, side):
    experts, width = code.shape
    slot = lax.broadcasted_iota(jnp.int32, (experts, 2 * SLOTS, width), 1).astype(F32)
    return (code[:, None, :] + float(side * SLOTS)) == slot


def norm(summed, gains, offset):
    average = jnp.mean(summed, axis=-1, keepdims=True)
    centred = summed - average
    spread = jnp.mean(centred * centred, axis=-1, keepdims=True)
    return centred * lax.rsqrt(spread + NORM_EPS) * gains + offset


def gated(gate_act, up_act):
    return (gate_act / (1.0 + jnp.exp(-gate_act)) * up_act).astype(BF16)


CHUNKS = 4


def group_peers(nx, core, x, z):
    me = core * nx + x
    peers = []
    for o in range(1, 2 * nx):
        i = lax.rem(me + o, 2 * nx)
        peers.append((i, {"sp": 2 * z + i // nx, "tp": lax.rem(i, nx)}))
    return me, peers


def dispatch_kernel(
    nz,
    nx,
    att_ref,
    wo_ref,
    res_ref,
    aux_ref,
    gain_ref,
    bias_ref,
    gate_hbm,
    up_hbm,
    down_hbm,
    sgate_hbm,
    sup_hbm,
    sdown_hbm,
    made_ref,
    base_ref,
    heads,
    rows_all,
    outgoing,
    slots,
    gate,
    up,
    down,
    sgate,
    sup,
    sdown,
    load_sem,
    head_send,
    head_recv,
    ring_send,
    ring_recv,
    slot_send,
    slot_recv,
):
    sp, z, core, x = place()
    nsp = 2 * nz
    tokens, width = res_ref.shape
    part = tokens // CHUNKS
    far_hop = nz // 2 - 1
    hop_to = (
        at_sp(lax.rem(sp + 2, nsp)),
        at_sp(lax.rem(sp + nsp - 2, nsp)),
    )
    me, peers = group_peers(nx, core, x, z)
    greet([hop_to[0], hop_to[1]] + [device for _, device in peers])

    def head_copy(o, to, at):
        return remote(
            att_ref.at[pl.ds(to * tokens, tokens)],
            heads.at[at],
            head_send.at[o - 1],
            head_recv.at[o - 1],
            {"tp": lax.rem(x + o, nx)},
        )

    for o in range(1, nx):
        head_copy(o, lax.rem(x + o, nx), x).start()

    loads = [
        pltpu.make_async_copy(src, dst, load_sem.at[n])
        for n, (src, dst) in enumerate(
            (
                (sgate_hbm, sgate),
                (sup_hbm, sup),
                (sdown_hbm, sdown),
                (gate_hbm, gate),
                (up_hbm, up),
                (down_hbm, down),
            )
        )
    ]
    for load in loads:
        load.start()

    heads[x] = att_ref[pl.ds(x * tokens, tokens), :]
    for o in range(1, nx):
        head_copy(o, x, lax.rem(x + nx - o, nx)).wait_recv()

    def source(way, s):
        return lax.rem(z + nz - (s + 1), nz) if way == 0 else lax.rem(z + s + 1, nz)

    def ring(way, s, c, block):
        piece = rows_all.at[block, pl.ds(c * part, part)]
        return remote(
            piece, piece, ring_send.at[way, s, c], ring_recv.at[way, s, c], hop_to[way]
        )

    by_token = jnp.concatenate([heads[i] for i in range(nx)], axis=1)
    mixed = jnp.dot(by_token, wo_ref[...], preferred_element_type=F32)
    normed = norm(
        res_ref[...].astype(F32) + mixed, gain_ref[...], bias_ref[...]
    ).astype(BF16)
    rows_all[z] = normed
    base_ref[...] = normed.astype(F32)

    for c in range(CHUNKS):
        for way in (0, 1):
            ring(way, 0, c, z).start()

    experts = 2 * nx

    def forward(s, block, way, c):
        ring(way, s, c, block).wait_recv()

    def chosen(block, side):
        code, _ = slot_codes(aux_ref[block], z, experts)
        picks = slot_matches(code, side)
        flat = jnp.where(picks, 1.0, 0.0).reshape(experts * 2 * SLOTS, tokens)
        return jnp.dot(flat.astype(BF16), rows_all[block], preferred_element_type=F32)

    def slot_copy(o, i, device, g, at):
        return remote(
            outgoing.at[i, g], slots.at[at, g], slot_send.at[o, g], slot_recv.at[o, g], device
        )

    def hand_out(first, second, g):
        found = chosen(first, 0) + chosen(second, 1)
        outgoing[:, g] = found.astype(BF16).reshape(experts, 2 * SLOTS, width)
        slots[me, g] = outgoing[me, g]
        for o, (i, device) in enumerate(peers):
            slot_copy(o, i, device, g, me).start()

    for load in loads[:3]:
        load.wait()
    own = rows_all[z]
    shared_hidden = gated(
        jnp.dot(own, sgate[...], preferred_element_type=F32),
        jnp.dot(own, sup[...], preferred_element_type=F32),
    )
    base_ref[...] += jnp.dot(shared_hidden, sdown[...], preferred_element_type=F32)

    @pl.loop(0, far_hop)
    def _(s):
        for c in range(CHUNKS):
            for way in (0, 1):
                block = source(way, s)
                ring(way, s, c, block).wait_recv()
                if (c < CHUNKS // 2) == (way == 0):
                    ring(way, s + 1, c, block).start()
                else:

                    @pl.when(s < far_hop - 1)
                    def _():
                        ring(way, s + 1, c, block).start()

        hand_out(source(0, s), source(1, s), s)

    for c in range(CHUNKS):
        way = 0 if c < CHUNKS // 2 else 1
        ring(way, far_hop, c, source(way, far_hop)).wait_recv()
    hand_out(source(0, far_hop), z, far_hop)

    for load in loads[3:]:
        load.wait()

    @pl.loop(0, nz // 2)
    def _(g):
        for o, (i, device) in enumerate(peers):
            slot_copy(o, i, device, g, i).wait_recv()

    together = 2
    lines = together * (nz // 2) * 2 * SLOTS

    @pl.loop(0, experts // together)
    def _(n):
        at = pl.ds(n * together, together)
        given = slots[at].reshape(lines, width)
        hidden = gated(
            jnp.dot(given, gate[0], preferred_element_type=F32),
            jnp.dot(given, up[0], preferred_element_type=F32),
        )
        made = jnp.dot(hidden, down[0], preferred_element_type=F32)
        made_ref[at] = made.astype(BF16).reshape(together, nz // 2, 2 * SLOTS, width)

    for o in range(1, nx):
        head_copy(o, x, x).wait_send()

    @pl.loop(0, far_hop)
    def _(s):
        for way in (0, 1):
            for c in range(CHUNKS):
                ring(way, s, c, z).wait_send()

    for c in range(CHUNKS):
        ring(0 if c < CHUNKS // 2 else 1, far_hop, c, z).wait_send()

    @pl.loop(0, nz // 2)
    def _(g):
        for o, (i, device) in enumerate(peers):
            slot_copy(o, i, device, g, i).wait_send()


def dispatch(nz, nx, att, wo, res, aux, gain, bias, weights, shared):
    tokens, width = res.shape
    groups = nz // 2
    experts = 2 * nx
    whole = pl.BlockSpec(memory_space=pltpu.VMEM)
    anywhere = pl.BlockSpec(memory_space=pl.ANY)
    dma = pltpu.SemaphoreType.DMA
    slot_shape = (experts, groups, 2 * SLOTS, width)
    return pl.pallas_call(
        functools.partial(dispatch_kernel, nz, nx),
        name="dispatch",
        out_shape=(
            jax.ShapeDtypeStruct(slot_shape, BF16),
            jax.ShapeDtypeStruct((tokens, width), F32),
        ),
        in_specs=[whole] * 6 + [anywhere] * 6,
        out_specs=(whole, whole),
        scratch_shapes=[
            pltpu.VMEM((nx, tokens, HEAD_DIM), BF16),
            pltpu.VMEM((nz, tokens, width), BF16),
            pltpu.VMEM(slot_shape, BF16),
            pltpu.VMEM(slot_shape, BF16),
            *[pltpu.VMEM(w.shape, BF16) for w in (*weights, *shared)],
            dma((6,)),
            dma((nx - 1,)),
            dma((nx - 1,)),
            dma((2, groups, CHUNKS)),
            dma((2, groups, CHUNKS)),
            dma((experts - 1, groups)),
            dma((experts - 1, groups)),
        ],
        compiler_params=pltpu.CompilerParams(collective_id=1, has_side_effects=True),
        cost_estimate=pl.CostEstimate(flops=1 << 33, bytes_accessed=1 << 24, transcendentals=0),
    )(att, wo, res, aux, gain, bias, *weights, *shared)


def collect_kernel(
    nz,
    nx,
    made_ref,
    base_ref,
    aux_ref,
    gain_ref,
    bias_ref,
    out_ref,
    back,
    held,
    sums,
    back_send,
    back_recv,
    ring_send,
    ring_recv,
):
    sp, z, core, x = place()
    nsp = 2 * nz
    tokens, width = base_ref.shape
    part = tokens // CHUNKS
    hops = nz // 2
    hop_to = (
        at_sp(lax.rem(sp + 2, nsp)),
        at_sp(lax.rem(sp + nsp - 2, nsp)),
    )
    me, peers = group_peers(nx, core, x, z)
    greet([hop_to[0], hop_to[1]] + [device for _, device in peers])
    experts = 2 * nx
    last = hops - 1

    def back_copy(o, i, device, g, at):
        return remote(
            made_ref.at[i, g], back.at[at, g], back_send.at[o, g], back_recv.at[o, g], device
        )

    @pl.loop(0, hops)
    def _(n):
        for o, (i, device) in enumerate(peers):
            back_copy(o, i, device, last - n, me).start()

    back[me] = made_ref[me]

    def arrived(g):
        for o, (i, device) in enumerate(peers):
            back_copy(o, i, device, g, i).wait_recv()

    def weighed(token_chip, side, g):
        code, share = slot_codes(aux_ref[token_chip], z, experts)
        picks = slot_matches(code, side)
        flat = jnp.where(picks, share[:, None, :], 0.0).reshape(experts * 2 * SLOTS, tokens)
        lines = back[:, g].reshape(experts * 2 * SLOTS, width)
        return jnp.dot(flat.T.astype(BF16), lines, preferred_element_type=F32)

    def ring(way, s, c):
        at = pl.ds(c * part, part)
        return remote(
            sums.at[way, s, at],
            held.at[way, s, at],
            ring_send.at[way, s, c],
            ring_recv.at[way, s, c],
            hop_to[way],
        )

    def first_half(c):
        return c < CHUNKS // 2

    def rows_of(c):
        return slice(c * part, (c + 1) * part)

    arrived(last)
    opposite = lax.rem(z + hops, nz)
    far = weighed(opposite, 0, last).astype(BF16)
    for c in range(CHUNKS):
        way = 0 if first_half(c) else 1
        sums[way, 0, rows_of(c), :] = far[rows_of(c), :]
        ring(way, 0, c).start()

    def step(s, received):
        g = last - s
        arrived(g)
        own = (
            weighed(lax.rem(z + hops - s, nz), 1, g),
            weighed(lax.rem(z + nz - hops + s, nz), 0, g),
        )
        for c in range(CHUNKS):
            for way in (0, 1):
                summed = own[way][rows_of(c), :]
                if received(way, c):
                    ring(way, s - 1, c).wait_recv()
                    summed = summed + held[way, s - 1, rows_of(c), :].astype(F32)
                sums[way, s, rows_of(c), :] = summed.astype(BF16)
                ring(way, s, c).start()

    step(1, lambda way, c: first_half(c) == (way == 0))

    @pl.loop(2, hops)
    def _(s):
        step(s, lambda way, c: True)

    base = base_ref[...] + weighed(z, 1, last)
    for c in range(CHUNKS):
        at = rows_of(c)
        for way in (0, 1):
            ring(way, last, c).wait_recv()
        summed = (
            base[at, :]
            + held[0, last, at, :].astype(F32)
            + held[1, last, at, :].astype(F32)
        )
        out_ref[at, :] = norm(summed, gain_ref[...], bias_ref[...]).astype(out_ref.dtype)

    for c in range(CHUNKS):
        ring(0 if first_half(c) else 1, 0, c).wait_send()

    @pl.loop(1, hops)
    def _(s):
        for way in (0, 1):
            for c in range(CHUNKS):
                ring(way, s, c).wait_send()

    @pl.loop(0, hops)
    def _(g):
        for o, (i, device) in enumerate(peers):
            back_copy(o, i, device, g, i).wait_send()


def collect(nz, nx, made, base, aux, gain, bias):
    tokens, width = base.shape
    hops = nz // 2
    experts = 2 * nx
    whole = pl.BlockSpec(memory_space=pltpu.VMEM)
    dma = pltpu.SemaphoreType.DMA
    return pl.pallas_call(
        functools.partial(collect_kernel, nz, nx),
        name="collect",
        out_shape=jax.ShapeDtypeStruct((tokens, width), BF16),
        in_specs=[whole] * 5,
        out_specs=whole,
        scratch_shapes=[
            pltpu.VMEM(made.shape, BF16),
            pltpu.VMEM((2, hops, tokens, width), BF16),
            pltpu.VMEM((2, hops, tokens, width), BF16),
            dma((experts - 1, hops)),
            dma((experts - 1, hops)),
            dma((2, hops, CHUNKS)),
            dma((2, hops, CHUNKS)),
        ],
        compiler_params=pltpu.CompilerParams(collective_id=2, has_side_effects=True),
        cost_estimate=pl.CostEstimate(flops=1 << 32, bytes_accessed=1 << 24, transcendentals=0),
    )(made, base, aux, gain, bias)


def local(
    query_rows,
    key_rows,
    value_rows,
    residual,
    output_weight,
    first_gain,
    first_bias,
    expert_ids,
    expert_share,
    gate_weight,
    up_weight,
    down_weight,
    shared_gate,
    shared_up,
    shared_down,
    second_gain,
    second_bias,
):
    nz = lax.axis_size("sp") // 2
    nx = lax.axis_size("tp")
    aux = jnp.concatenate([expert_ids.T.astype(F32), expert_share.T], axis=0)
    attended, wo, aux_all = attention(
        nz, nx, query_rows, key_rows, value_rows, output_weight, aux
    )
    made, base = dispatch(
        nz,
        nx,
        attended,
        wo,
        residual,
        aux_all,
        first_gain[None, :],
        first_bias[None, :],
        (gate_weight, up_weight, down_weight),
        (shared_gate, shared_up, shared_down),
    )
    return collect(nz, nx, made, base, aux_all, second_gain[None, :], second_bias[None, :])


def solution(mesh):
    return jax.shard_map(
        local,
        mesh=mesh,
        in_specs=(
            P(("grp", "sp"), "tp"),
            P(("grp", "sp"), "tp"),
            P(("grp", "sp"), "tp"),
            P(("grp", "sp", "tp"), None),
            P("tp", None),
            P(),
            P(),
            P(("grp", "sp", "tp"), None),
            P(("grp", "sp", "tp"), None),
            P(("sp", "tp"), None, None),
            P(("sp", "tp"), None, None),
            P(("sp", "tp"), None, None),
            P(),
            P(),
            P(),
            P(),
            P(),
        ),
        out_specs=P(("grp", "sp", "tp"), None),
        check_vma=False,
    )
```

```python
import functools

import jax
import jax.numpy as jnp
from jax import lax
from jax.experimental import pallas as pl
from jax.experimental.pallas import tpu as pltpu
from jax.sharding import PartitionSpec as P

HEAD_DIM = 128
KBLK = 128
NORM_EPS = 1e-05
LOG2E = 1.4426950408889634
MESH = pl.DeviceIdType.MESH
SLOTS = 8
USED = 6
BF16 = jnp.bfloat16
F32 = jnp.float32


def at_sp(sp):
    return {"sp": sp}


def place():
    sp = lax.axis_index("sp")
    return sp, sp // 2, sp % 2, lax.axis_index("tp")


def greet(devices):
    barrier = pltpu.get_barrier_semaphore()
    for device in devices:
        pl.semaphore_signal(barrier, inc=1, device_id=device, device_id_type=MESH)
    pl.semaphore_wait(barrier, len(devices))


def remote(src, dst, send_sem, recv_sem, device):
    return pltpu.make_async_remote_copy(
        src_ref=src,
        dst_ref=dst,
        send_sem=send_sem,
        recv_sem=recv_sem,
        device_id=device,
        device_id_type=MESH,
    )


def slot_codes(aux, z, experts):
    width = aux.shape[1]
    picks = aux.shape[0] // 2
    number = (z * experts + lax.broadcasted_iota(jnp.int32, (experts, width), 0)).astype(F32)
    named = jnp.zeros((experts, width), F32)
    share = jnp.zeros((experts, width), F32)
    for k in range(picks):
        hit = aux[k : k + 1, :] == number
        named = named + jnp.where(hit, 1.0, 0.0)
        share = share + jnp.where(hit, aux[picks + k : picks + k + 1, :], 0.0)
    earlier = lax.broadcasted_iota(jnp.int32, (width, width), 0)
    later = lax.broadcasted_iota(jnp.int32, (width, width), 1)
    before = (earlier < later).astype(F32).astype(BF16)
    rank = jnp.dot(named.astype(BF16), before, preferred_element_type=F32)
    return jnp.where(named > 0.0, rank, -1000.0), share


def slot_matches(code, side):
    experts, width = code.shape
    slot = lax.broadcasted_iota(jnp.int32, (experts, 2 * SLOTS, width), 1).astype(F32)
    return (code[:, None, :] + float(side * SLOTS)) == slot


def norm(summed, gains, offset):
    average = jnp.mean(summed, axis=-1, keepdims=True)
    centred = summed - average
    spread = jnp.mean(centred * centred, axis=-1, keepdims=True)
    return centred * lax.rsqrt(spread + NORM_EPS) * gains + offset


def gated(gate_act, up_act):
    return (gate_act / (1.0 + jnp.exp(-gate_act)) * up_act).astype(BF16)


CHUNKS = 4


def group_peers(nx, core, x, z):
    me = core * nx + x
    peers = []
    for o in range(1, 2 * nx):
        i = lax.rem(me + o, 2 * nx)
        peers.append((i, {"sp": 2 * z + i // nx, "tp": lax.rem(i, nx)}))
    return me, peers


class Names:
    pass


def layer_kernel(nz, nx, *refs):
    sp, z, core, x = place()
    nsp = 2 * nz
    r = Names()
    for name, ref in zip(REFS, refs, strict=True):
        setattr(r, name, ref)
    hop_to = (at_sp(lax.rem(sp + 2, nsp)), at_sp(lax.rem(sp + nsp - 2, nsp)))
    partner = at_sp(sp + 1 - 2 * core)
    across = [{"tp": lax.rem(x + o, nx)} for o in range(1, nx)]
    me, peers = group_peers(nx, core, x, z)

    def shift(way, by):
        return lax.rem(z + by, nz) if way == 0 else lax.rem(z + nz - by, nz)

    def member(chip, i):
        return {"sp": 2 * chip + i // nx, "tp": i % nx}

    r.raw_in[...] = jnp.zeros_like(r.raw_in)
    greet(
        [device for _, device in peers]
        + [
            member(shift(way, by), i)
            for by in (1, 2)
            for way in (0, 1)
            for i in range(2 * nx)
        ]
    )

    hops = nz // 2
    last = hops - 1
    experts = 2 * nx
    tokens, width = r.res.shape
    rows = r.q.shape[0]

    loads = [
        pltpu.make_async_copy(src, dst, r.load_sem.at[n])
        for n, (src, dst) in enumerate(
            (
                (r.sgate_hbm, r.sgate),
                (r.sup_hbm, r.sup),
                (r.sdown_hbm, r.sdown),
                (r.gate_hbm, r.gate),
                (r.up_hbm, r.up),
                (r.down_hbm, r.down),
            )
        )
    ]

    def source(way, s):
        return lax.rem(z + nz - (s + 1), nz) if way == 0 else lax.rem(z + s + 1, nz)


    half = rows // 2
    wo_rows = r.wo.shape[0]

    def piece(block, c):
        return r.kv.at[c // 2, block, pl.ds((c % 2) * half, half)]

    def own_piece(c):
        return (r.k, r.v)[c // 2].at[pl.ds((c % 2) * half, half)]

    def ring(way, s, c, block, src=None):
        return remote(
            piece(block, c) if src is None else src,
            piece(block, c),
            r.kv_send.at[way, s, c],
            r.kv_recv.at[way, s, c],
            hop_to[way],
        )

    def pair(way, s, c, block):
        return remote(
            piece(block, c),
            piece(block, c),
            r.pair_send.at[way, s, c],
            r.pair_recv.at[way, s, c],
            partner,
        )

    def own_pair(c, block):
        return remote(own_piece(c), piece(block, c), r.own_send.at[c], r.own_recv.at[c], partner)

    def aux_hop(way, s, block, src=None):
        return remote(
            r.aux_all.at[block] if src is None else src,
            r.aux_all.at[block],
            r.aux_send.at[way, s],
            r.aux_recv.at[way, s],
            hop_to[way],
        )

    def wo_copy(o, at):
        return remote(
            r.wo,
            r.wo_all.at[pl.ds(at * wo_rows, wo_rows)],
            r.wo_send.at[o - 1],
            r.wo_recv.at[o - 1],
            across[o - 1],
        )

    for way in (0, 1):
        aux_hop(way, 0, z, r.aux).start()
    for c in range(4):
        for way in (0, 1):
            ring(way, 0, c, sp, own_piece(c)).start()
        own_pair(c, sp).start()
    for o in range(1, nx):
        wo_copy(o, x).start()
    for load in loads:
        load.start()

    r.kv[0, sp] = r.k[...]
    r.kv[1, sp] = r.v[...]
    r.aux_all[z] = r.aux[...]
    r.wo_all[pl.ds(x * wo_rows, wo_rows), :] = r.wo[...]
    r.acc[...] = jnp.zeros_like(r.acc)
    r.behind[...] = jnp.zeros_like(r.behind)
    r.far[...] = jnp.zeros_like(r.far)

    tile = min(256, rows)
    above = lax.broadcasted_iota(jnp.int32, (KBLK, 2 * KBLK), 0)
    below = lax.broadcasted_iota(jnp.int32, (KBLK, 2 * KBLK), 1)
    sums = ((above > below) | (below >= KBLK)).astype(F32).astype(BF16)
    to_log2 = HEAD_DIM ** (-0.5) * LOG2E

    def visit(block, mode):
        @pl.loop(0, rows // tile)
        def _(t):
            here = pl.ds(pl.multiple_of(t * tile, tile), tile)
            q = r.q[here, :]
            spent_after = (
                jnp.zeros((tile, KBLK), F32) if mode == "far" else r.behind[here, :]
            )
            total = jnp.zeros((tile, HEAD_DIM), F32)
            for b in reversed(range(rows // KBLK)):
                span = pl.ds(b * KBLK, KBLK)
                score = (
                    lax.dot_general(
                        q,
                        r.kv[0, block, span, :],
                        (((1,), (1,)), ((), ())),
                        preferred_element_type=F32,
                    )
                    * to_log2
                )
                soft = jnp.maximum(
                    score, jnp.log(1.0 + jnp.exp2(jnp.minimum(score, 64.0))) * LOG2E
                )
                if mode == "diagonal":
                    key_pos = b * KBLK + lax.broadcasted_iota(jnp.int32, (tile, KBLK), 1)
                    query_pos = t * tile + lax.broadcasted_iota(jnp.int32, (tile, KBLK), 0)
                    usable = key_pos < query_pos
                    spent = jnp.where(usable, soft, 0.0)
                else:
                    spent = soft
                added = jnp.dot(spent.astype(BF16), sums, preferred_element_type=F32)
                weight = jnp.exp2(((score - soft) - added[:, :KBLK]) - spent_after)
                if mode == "diagonal":
                    weight = jnp.where(usable, weight, 0.0)
                spent_after = spent_after + added[:, KBLK:]
                total = total + jnp.dot(
                    weight.astype(BF16), r.kv[1, block, span, :], preferred_element_type=F32
                )
            if mode == "far":
                r.far[here, :] = r.far[here, :] * jnp.exp2(-spent_after) + total
            else:
                r.acc[here, :] = r.acc[here, :] + total
                r.behind[here, :] = spent_after

    def work(s, c):
        near_chip = z - (s + 1)
        far_chip = z + s + 1 - nz
        if c < 2:

            @pl.when(near_chip >= 0)
            def _():
                visit(jnp.maximum(2 * near_chip + 1 - c, 0), "near")

        else:

            @pl.when(far_chip >= 0)
            def _():
                visit(jnp.maximum(2 * far_chip + c - 2, 0), "far")

    def of_pair(way, s):
        return 2 * source(way, s) + 1 - core

    visit(sp, "diagonal")
    other = sp + 1 - 2 * core
    for c in range(4):
        own_pair(c, other).wait_recv()

    @pl.when(core == 1)
    def _():
        visit(other, "near")

    @pl.loop(0, last)
    def _(s):
        for way in (0, 1):
            aux_hop(way, s, source(way, s)).wait_recv()

            @pl.when((s < last - 1) | (way == 0))
            def _():
                aux_hop(way, s + 1, source(way, s)).start()

        for c in range(4):
            for way in (0, 1):
                block = 2 * source(way, s) + core
                ring(way, s, c, block).wait_recv()
                if (c < 2) == (way == 0):
                    ring(way, s + 1, c, block).start()
                else:

                    @pl.when(s < last - 1)
                    def _():
                        ring(way, s + 1, c, block).start()

                pair(way, s, c, block).start()

            @pl.when(s > 0)
            def _():
                if c == 0:
                    for way in (0, 1):
                        for c2 in range(4):
                            pair(way, s - 1, c2, of_pair(way, s - 1)).wait_recv()
                work(s - 1, c)

    for way in (0, 1):
        for c2 in range(4):
            pair(way, last - 1, c2, of_pair(way, last - 1)).wait_recv()
    for c in range(4):
        work(last - 1, c)
    aux_hop(0, last, source(0, last)).wait_recv()
    for c in range(4):
        way = c // 2
        block = 2 * source(way, last) + core
        ring(way, last, c, block).wait_recv()
        pair(way, last, c, block).start()
    for c in range(4):
        way = c // 2
        pair(way, last, c, of_pair(way, last)).wait_recv()
    for c in range(2):
        work(last, c)
    r.att[...] = (r.acc[...] + r.far[...] * jnp.exp2(-r.behind[...])).astype(BF16)


    def head_copy(o, to, at):
        return remote(
            r.att.at[pl.ds(to * tokens, tokens)],
            r.heads.at[at],
            r.head_send.at[o - 1],
            r.head_recv.at[o - 1],
            across[o - 1],
        )

    for o in range(1, nx):
        head_copy(o, lax.rem(x + o, nx), x).start()
    r.heads[x] = r.att[pl.ds(x * tokens, tokens), :]
    for o in range(1, nx):
        wo_copy(o, lax.rem(x + nx - o, nx)).wait_recv()
    for o in range(1, nx):
        head_copy(o, x, lax.rem(x + nx - o, nx)).wait_recv()
    by_token = jnp.concatenate([r.heads[i] for i in range(nx)], axis=1)
    mixed = jnp.dot(by_token, r.wo_all[...], preferred_element_type=F32)
    normed = norm(r.res[...].astype(F32) + mixed, r.gain1[...], r.bias1[...]).astype(BF16)
    r.rows_all[z] = normed


    part = tokens // CHUNKS

    def row_ring(way, s, c, block):
        at = r.rows_all.at[block, pl.ds(c * part, part)]
        return remote(at, at, r.row_send.at[way, s, c], r.row_recv.at[way, s, c], hop_to[way])

    for c in range(CHUNKS):
        for way in (0, 1):
            row_ring(way, 0, c, z).start()
    r.base[...] = r.rows_all[z].astype(F32)

    def chosen(block, side):
        code, _ = slot_codes(r.aux_all[block], z, experts)
        flat = jnp.where(slot_matches(code, side), 1.0, 0.0)
        flat = flat.reshape(experts * 2 * SLOTS, tokens).astype(BF16)
        return jnp.dot(flat, r.rows_all[block], preferred_element_type=F32)

    def outgoing_slot(g):
        return lax.rem(g, 2) if not isinstance(g, int) or g < last else 2

    def slot_copy(o, i, device, g, at, side=None):
        lines = pl.ds(0, 2 * SLOTS) if side is None else pl.ds(side * SLOTS, SLOTS)
        sem = g if side is None else last + side
        return remote(
            r.outgoing.at[i, outgoing_slot(g), lines],
            r.slots.at[at, g, lines],
            r.slot_send.at[o, sem],
            r.slot_recv.at[o, sem],
            device,
        )

    def send_slots(g):
        r.slots[me, g] = r.outgoing[me, outgoing_slot(g)]
        for o, (i, device) in enumerate(peers):
            slot_copy(o, i, device, g, me).start()

    def send_side(found, side):
        lines = slice(side * SLOTS, (side + 1) * SLOTS)
        found = found.astype(BF16).reshape(experts, 2 * SLOTS, width)
        r.outgoing[:, 2, lines] = found[:, lines]
        r.slots[me, last, lines] = r.outgoing[me, 2, lines]
        for o, (i, device) in enumerate(peers):
            slot_copy(o, i, device, last, me, side).start()

    def slots_sent(g):
        for o, (i, device) in enumerate(peers):
            slot_copy(o, i, device, g, i).wait_send()

    def fill(found, g):
        r.outgoing[:, outgoing_slot(g)] = found.astype(BF16).reshape(
            experts, 2 * SLOTS, width
        )
        send_slots(g)

    def back_copy(o, i, device, g, at, side=None):
        lines = pl.ds(0, 2 * SLOTS) if side is None else pl.ds(side * SLOTS, SLOTS)
        return remote(
            r.slots.at[i, g, lines],
            r.back.at[at, g, lines],
            r.back_send.at[o, g],
            r.back_recv.at[o, g],
            device,
        )

    def give_back(g, side=None):
        lines = slice(0, 2 * SLOTS) if side is None else slice(side * SLOTS, (side + 1) * SLOTS)
        r.back[me, g, lines] = r.slots[me, g, lines]
        for o, (i, device) in enumerate(peers):
            back_copy(o, i, device, g, me, side).start()

    def produce(g):
        given = r.slots[:, g].reshape(experts * 2 * SLOTS, width)
        hidden = gated(
            jnp.dot(given, r.gate[0], preferred_element_type=F32),
            jnp.dot(given, r.up[0], preferred_element_type=F32),
        )
        made = jnp.dot(hidden, r.down[0], preferred_element_type=F32)
        r.slots[:, g] = made.astype(BF16).reshape(experts, 2 * SLOTS, width)

    def serve(g):
        for o, (i, device) in enumerate(peers):
            slot_copy(o, i, device, g, i).wait_recv()
        produce(g)


    taken = pl.ds(0, USED)

    def far_send(way, n):
        chip = shift(way, 1) if n < experts else shift(way, 2)
        i = n if n < experts else way * nx + n - experts
        lines = pl.ds(way * SLOTS if n < experts else 0, USED)
        row = way if n < experts else 2
        return remote(
            r.far_out.at[way, n, taken],
            r.slots.at[me, last - 1 if n < experts else last, lines],
            r.far_send.at[way, n],
            r.far_recv.at[row, me],
            member(chip, i),
        )

    def far_arrival(row, i):
        side = row if row < 2 else 0
        here = r.slots.at[i, last - 1 if row < 2 else last, pl.ds(side * SLOTS, USED)]
        return remote(
            r.far_out.at[0, 0, taken], here, r.far_send.at[0, 0], r.far_recv.at[row, i], hop_to[0]
        )

    def far_return(row, i):
        way = row if row < 2 else core
        if row < 2:
            chip, n = shift(1 - row, 1), me
        else:
            chip, n = lax.rem(z + nz - 2 + 4 * core, nz), experts + x
        side = row if row < 2 else 0
        return remote(
            r.slots.at[i, last - 1 if row < 2 else last, pl.ds(side * SLOTS, USED)],
            r.raw_in.at[way, n, taken],
            r.raw_send.at[row, i],
            r.raw_recv.at[way, n],
            member(chip, i),
        )

    def raw_arrival(way, n):
        return remote(
            r.far_out.at[0, 0, taken],
            r.raw_in.at[way, n, taken],
            r.far_send.at[0, 0],
            r.raw_recv.at[way, n],
            hop_to[0],
        )

    def far_codes(way):
        aux = r.aux_all[source(way, last - 2)]
        code_one, share_one = slot_codes(aux, shift(way, 1), experts)
        code_two, share_two = slot_codes(aux, shift(way, 2), experts)
        part_two = slice(way * nx, (way + 1) * nx)
        code = jnp.concatenate([code_one, code_two[part_two]], axis=0)
        share = jnp.concatenate([share_one, share_two[part_two]], axis=0)
        slot = lax.broadcasted_iota(jnp.int32, (experts + nx, SLOTS, tokens), 1).astype(F32)
        return code[:, None, :] == slot, share[:, None, :]

    many = (experts + nx) * SLOTS

    def pass_on(way):
        picks, _ = far_codes(way)
        flat = jnp.where(picks, 1.0, 0.0).reshape(many, tokens).astype(BF16)
        found = jnp.dot(flat, r.rows_all[source(way, last - 2)], preferred_element_type=F32)
        r.far_out[way] = found.astype(BF16).reshape(experts + nx, SLOTS, width)
        for n in reversed(range(experts + nx)):
            far_send(way, n).start()

    for load in loads[:3]:
        load.wait()
    own = r.rows_all[z]
    shared_hidden = gated(
        jnp.dot(own, r.sgate[...], preferred_element_type=F32),
        jnp.dot(own, r.sup[...], preferred_element_type=F32),
    )
    r.base[...] += jnp.dot(shared_hidden, r.sdown[...], preferred_element_type=F32)
    send_side(chosen(z, 1), 1)
    for load in loads[3:]:
        load.wait()

    @pl.loop(0, last - 1)
    def _(s):
        for c in range(CHUNKS):
            for way in (0, 1):
                block = source(way, s)
                row_ring(way, s, c, block).wait_recv()

                @pl.when(s < last - 2)
                def _():
                    row_ring(way, s + 1, c, block).start()

        @pl.when(s == last - 2)
        def _():
            for way in (0, 1):
                pass_on(way)

        @pl.when(s > 1)
        def _():
            slots_sent(s - 2)

        fill(chosen(source(0, s), 0) + chosen(source(1, s), 1), s)

        @pl.when(s > 0)
        def _():
            serve(s - 1)

    serve(last - 2)
    for o, (i, device) in enumerate(peers):
        slot_copy(o, i, device, last, i, 1).wait_recv()
    for i in range(experts):
        far_arrival(2, i).wait_recv()
    produce(last)
    for i in range(experts):
        far_return(2, i).start()
    for row in (0, 1):
        for i in range(experts):
            far_arrival(row, i).wait_recv()
    produce(last - 1)
    for row in (0, 1):
        for i in range(experts):
            far_return(row, i).start()
    for g in (last - 2, last - 3, last - 4):
        give_back(g)
    give_back(last, 1)


    def arrived(g, side=None):
        for o, (i, device) in enumerate(peers):
            back_copy(o, i, device, g, i, side).wait_recv()

    def lines_of(g):
        return r.back[:, g].reshape(experts * 2 * SLOTS, width)

    def weighed(token_chip, side, g):
        code, share = slot_codes(r.aux_all[token_chip], z, experts)
        flat = jnp.where(slot_matches(code, side), share[:, None, :], 0.0)
        flat = flat.reshape(experts * 2 * SLOTS, tokens)
        return jnp.dot(flat.T.astype(BF16), lines_of(g), preferred_element_type=F32)

    def sum_ring(way, s, c):
        at = pl.ds(c * part, part)
        return remote(
            r.sums.at[way, s - 2, at],
            r.held.at[way, s - 2, at],
            r.sum_send.at[way, s - 2, c],
            r.sum_recv.at[way, s - 2, c],
            hop_to[way],
        )

    def part_of(c):
        return slice(c * part, (c + 1) * part)

    def target(way, s):
        return lax.rem(z + hops - s, nz) if way == 0 else lax.rem(z + nz - hops + s, nz)

    def from_far(way):
        picks, share = far_codes(1 - way)
        flat = jnp.where(picks, share, 0.0).reshape(many, tokens)
        lines = r.raw_in[1 - way].reshape(many, width)
        return jnp.dot(flat.T.astype(BF16), lines, preferred_element_type=F32)

    arrived(last - 2)
    near = [weighed(target(way, 2), 1 - way, last - 2) for way in (0, 1)]
    for way in (0, 1):
        for n in range(experts + nx):
            raw_arrival(1 - way, n).wait_recv()
        summed = near[way] + from_far(way)
        r.sums[way, 0] = summed.astype(BF16)
        for c in range(CHUNKS):
            sum_ring(way, 2, c).start()

    @pl.loop(3, hops)
    def _(s):
        g = last - s

        @pl.when(g > 1)
        def _():
            give_back(g - 2)

        arrived(g)
        mine = [weighed(target(way, s), 1 - way, g) for way in (0, 1)]
        for c in range(CHUNKS):
            for way in (0, 1):
                sum_ring(way, s - 1, c).wait_recv()
                summed = mine[way][part_of(c), :] + r.held[way, s - 3, part_of(c), :].astype(F32)
                r.sums[way, s - 2, part_of(c), :] = summed.astype(BF16)
                sum_ring(way, s, c).start()

    arrived(last, 1)
    code, share = slot_codes(r.aux_all[z], z, experts)
    slot = lax.broadcasted_iota(jnp.int32, (experts, SLOTS, tokens), 1).astype(F32)
    flat = jnp.where(code[:, None, :] == slot, share[:, None, :], 0.0)
    r.base[...] += jnp.dot(
        flat.reshape(experts * SLOTS, tokens).T.astype(BF16),
        r.back[:, last, SLOTS:].reshape(experts * SLOTS, width),
        preferred_element_type=F32,
    )
    for c in range(CHUNKS):
        for way in (0, 1):
            sum_ring(way, last, c).wait_recv()
        summed = (
            r.base[part_of(c), :]
            + r.held[0, last - 2, part_of(c), :].astype(F32)
            + r.held[1, last - 2, part_of(c), :].astype(F32)
        )
        r.out[part_of(c), :] = norm(summed, r.gain2[...], r.bias2[...]).astype(r.out.dtype)


    for o in range(1, nx):
        wo_copy(o, x).wait_send()
        head_copy(o, x, x).wait_send()
    for c in range(4):
        own_pair(c, sp).wait_send()

    @pl.loop(0, last)
    def _(s):
        for way in (0, 1):
            aux_hop(way, s, z).wait_send()
            for c in range(4):
                ring(way, s, c, sp).wait_send()
                pair(way, s, c, sp).wait_send()

    aux_hop(0, last, z).wait_send()
    for c in range(4):
        ring(c // 2, last, c, sp).wait_send()
        pair(c // 2, last, c, sp).wait_send()

    @pl.loop(0, last - 1)
    def _(s):
        for way in (0, 1):
            for c in range(CHUNKS):
                row_ring(way, s, c, z).wait_send()
                sum_ring(way, s + 2, c).wait_send()

    for way in (0, 1):
        for n in range(experts + nx):
            far_send(way, n).wait_send()
    for row in range(3):
        for i in range(experts):
            far_return(row, i).wait_send()
    slots_sent(last - 3)
    slots_sent(last - 2)
    for o, (i, device) in enumerate(peers):
        slot_copy(o, i, device, last, i, 1).wait_send()
        back_copy(o, i, device, last, i, 1).wait_send()

    @pl.loop(0, last - 1)
    def _(g):
        for o, (i, device) in enumerate(peers):
            back_copy(o, i, device, g, i).wait_send()


REFS = (
    "q",
    "k",
    "v",
    "wo",
    "aux",
    "res",
    "gain1",
    "bias1",
    "gain2",
    "bias2",
    "gate_hbm",
    "up_hbm",
    "down_hbm",
    "sgate_hbm",
    "sup_hbm",
    "sdown_hbm",
    "out",
    "kv",
    "acc",
    "behind",
    "far",
    "aux_all",
    "wo_all",
    "att",
    "heads",
    "rows_all",
    "base",
    "outgoing",
    "slots",
    "back",
    "gate",
    "up",
    "down",
    "sgate",
    "sup",
    "sdown",
    "far_out",
    "raw_in",
    "sums",
    "held",
    "load_sem",
    "kv_send",
    "kv_recv",
    "pair_send",
    "pair_recv",
    "own_send",
    "own_recv",
    "aux_send",
    "aux_recv",
    "wo_send",
    "wo_recv",
    "head_send",
    "head_recv",
    "row_send",
    "row_recv",
    "slot_send",
    "slot_recv",
    "back_send",
    "back_recv",
    "far_send",
    "far_recv",
    "raw_send",
    "raw_recv",
    "sum_send",
    "sum_recv",
)


def layer(nz, nx, q, k, v, wo, aux, res, norms, weights, shared):
    rows, head = q.shape
    tokens, width = res.shape
    hops = nz // 2
    experts = 2 * nx
    whole = pl.BlockSpec(memory_space=pltpu.VMEM)
    anywhere = pl.BlockSpec(memory_space=pl.ANY)
    dma = pltpu.SemaphoreType.DMA
    slot_shape = (experts, hops, 2 * SLOTS, width)
    return pl.pallas_call(
        functools.partial(layer_kernel, nz, nx),
        name="layer",
        out_shape=jax.ShapeDtypeStruct((tokens, width), BF16),
        in_specs=[whole] * 10 + [anywhere] * 6,
        out_specs=whole,
        scratch_shapes=[
            pltpu.VMEM((2, 2 * nz, rows, head), BF16),
            pltpu.VMEM((rows, head), F32),
            pltpu.VMEM((rows, KBLK), F32),
            pltpu.VMEM((rows, head), F32),
            pltpu.VMEM((nz, *aux.shape), F32),
            pltpu.VMEM((nx * wo.shape[0], width), BF16),
            pltpu.VMEM((rows, head), BF16),
            pltpu.VMEM((nx, tokens, head), BF16),
            pltpu.VMEM((nz, tokens, width), BF16),
            pltpu.VMEM((tokens, width), F32),
            pltpu.VMEM((experts, 3, 2 * SLOTS, width), BF16),
            pltpu.VMEM(slot_shape, BF16),
            pltpu.VMEM(slot_shape, BF16),
            *[pltpu.VMEM(w.shape, BF16) for w in (*weights, *shared)],
            pltpu.VMEM((2, experts + nx, SLOTS, width), BF16),
            pltpu.VMEM((2, experts + nx, SLOTS, width), BF16),
            pltpu.VMEM((2, hops - 2, tokens, width), BF16),
            pltpu.VMEM((2, hops - 2, tokens, width), BF16),
            dma((6,)),
            dma((2, hops, 4)),
            dma((2, hops, 4)),
            dma((2, hops, 4)),
            dma((2, hops, 4)),
            dma((4,)),
            dma((4,)),
            dma((2, hops)),
            dma((2, hops)),
            dma((nx - 1,)),
            dma((nx - 1,)),
            dma((nx - 1,)),
            dma((nx - 1,)),
            dma((2, hops - 2, CHUNKS)),
            dma((2, hops - 2, CHUNKS)),
            dma((experts - 1, hops + 1)),
            dma((experts - 1, hops + 1)),
            dma((experts - 1, hops)),
            dma((experts - 1, hops)),
            dma((2, experts + nx)),
            dma((3, experts)),
            dma((3, experts)),
            dma((2, experts + nx)),
            dma((2, hops - 2, CHUNKS)),
            dma((2, hops - 2, CHUNKS)),
        ],
        compiler_params=pltpu.CompilerParams(
            collective_id=0, has_side_effects=True, vmem_limit_bytes=67_000_000
        ),
        cost_estimate=pl.CostEstimate(flops=1 << 34, bytes_accessed=1 << 24, transcendentals=0),
    )(q, k, v, wo, aux, res, *norms, *weights, *shared)


def local(
    query_rows,
    key_rows,
    value_rows,
    residual,
    output_weight,
    first_gain,
    first_bias,
    expert_ids,
    expert_share,
    gate_weight,
    up_weight,
    down_weight,
    shared_gate,
    shared_up,
    shared_down,
    second_gain,
    second_bias,
):
    nz = lax.axis_size("sp") // 2
    nx = lax.axis_size("tp")
    aux = jnp.concatenate([expert_ids.T.astype(F32), expert_share.T], axis=0)
    norms = [a[None, :] for a in (first_gain, first_bias, second_gain, second_bias)]
    return layer(
        nz,
        nx,
        query_rows,
        key_rows,
        value_rows,
        output_weight,
        aux,
        residual,
        norms,
        (gate_weight, up_weight, down_weight),
        (shared_gate, shared_up, shared_down),
    )


def solution(mesh):
    return jax.shard_map(
        local,
        mesh=mesh,
        in_specs=(
            P(("grp", "sp"), "tp"),
            P(("grp", "sp"), "tp"),
            P(("grp", "sp"), "tp"),
            P(("grp", "sp", "tp"), None),
            P("tp", None),
            P(),
            P(),
            P(("grp", "sp", "tp"), None),
            P(("grp", "sp", "tp"), None),
            P(("sp", "tp"), None, None),
            P(("sp", "tp"), None, None),
            P(("sp", "tp"), None, None),
            P(),
            P(),
            P(),
            P(),
            P(),
        ),
        out_specs=P(("grp", "sp", "tp"), None),
        check_vma=False,
    )
```

```python
import functools

import jax
import jax.numpy as jnp
from jax import lax
from jax.experimental import pallas as pl
from jax.experimental.pallas import tpu as pltpu
from jax.sharding import PartitionSpec as P

HEAD_DIM = 128
KBLK = 128
NORM_EPS = 1e-05
LOG2E = 1.4426950408889634
MESH = pl.DeviceIdType.MESH
SLOTS = 8
USED = 6
BF16 = jnp.bfloat16
F32 = jnp.float32


def at_sp(sp):
    return {"sp": sp}


def place():
    sp = lax.axis_index("sp")
    return sp, sp // 2, sp % 2, lax.axis_index("tp")


def greet(devices):
    barrier = pltpu.get_barrier_semaphore()
    for device in devices:
        pl.semaphore_signal(barrier, inc=1, device_id=device, device_id_type=MESH)
    pl.semaphore_wait(barrier, len(devices))


def remote(src, dst, send_sem, recv_sem, device):
    return pltpu.make_async_remote_copy(
        src_ref=src,
        dst_ref=dst,
        send_sem=send_sem,
        recv_sem=recv_sem,
        device_id=device,
        device_id_type=MESH,
    )


def slot_codes(aux, z, experts):
    width = aux.shape[1]
    picks = aux.shape[0] // 2
    number = (z * experts + lax.broadcasted_iota(jnp.int32, (experts, width), 0)).astype(F32)
    named = jnp.zeros((experts, width), F32)
    share = jnp.zeros((experts, width), F32)
    for k in range(picks):
        hit = aux[k : k + 1, :] == number
        named = named + jnp.where(hit, 1.0, 0.0)
        share = share + jnp.where(hit, aux[picks + k : picks + k + 1, :], 0.0)
    earlier = lax.broadcasted_iota(jnp.int32, (width, width), 0)
    later = lax.broadcasted_iota(jnp.int32, (width, width), 1)
    before = (earlier < later).astype(F32).astype(BF16)
    rank = jnp.dot(named.astype(BF16), before, preferred_element_type=F32)
    return jnp.where(named > 0.0, rank, -1000.0), share


def slot_matches(code, side):
    experts, width = code.shape
    slot = lax.broadcasted_iota(jnp.int32, (experts, 2 * SLOTS, width), 1).astype(F32)
    return (code[:, None, :] + float(side * SLOTS)) == slot


def norm(summed, gains, offset):
    average = jnp.mean(summed, axis=-1, keepdims=True)
    centred = summed - average
    spread = jnp.mean(centred * centred, axis=-1, keepdims=True)
    return centred * lax.rsqrt(spread + NORM_EPS) * gains + offset


def gated(gate_act, up_act):
    return (gate_act / (1.0 + jnp.exp(-gate_act)) * up_act).astype(BF16)


CHUNKS = 4


def group_peers(nx, core, x, z):
    me = core * nx + x
    peers = []
    for o in range(1, 2 * nx):
        i = lax.rem(me + o, 2 * nx)
        peers.append((i, {"sp": 2 * z + i // nx, "tp": lax.rem(i, nx)}))
    return me, peers


class Names:
    pass


def layer_kernel(nz, nx, *refs):
    sp, z, core, x = place()
    nsp = 2 * nz
    r = Names()
    for name, ref in zip(REFS, refs, strict=True):
        setattr(r, name, ref)
    hop_to = (at_sp(lax.rem(sp + 2, nsp)), at_sp(lax.rem(sp + nsp - 2, nsp)))
    partner = at_sp(sp + 1 - 2 * core)
    across = [{"tp": lax.rem(x + o, nx)} for o in range(1, nx)]
    me, peers = group_peers(nx, core, x, z)

    def shift(way, by):
        return lax.rem(z + by, nz) if way == 0 else lax.rem(z + nz - by, nz)

    def member(chip, i):
        return {"sp": 2 * chip + i // nx, "tp": i % nx}

    r.raw_in[...] = jnp.zeros_like(r.raw_in)
    greet(
        [device for _, device in peers]
        + [
            member(shift(way, by), i)
            for by in (1, 2)
            for way in (0, 1)
            for i in range(2 * nx)
        ]
    )

    hops = nz // 2
    last = hops - 1
    experts = 2 * nx
    tokens, width = r.res.shape
    rows = r.q.shape[0]

    loads = [
        pltpu.make_async_copy(src, dst, r.load_sem.at[n])
        for n, (src, dst) in enumerate(
            (
                (r.sgate_hbm, r.sgate),
                (r.sup_hbm, r.sup),
                (r.sdown_hbm, r.sdown),
                (r.gate_hbm, r.gate),
                (r.up_hbm, r.up),
                (r.down_hbm, r.down),
            )
        )
    ]

    def source(way, s):
        return lax.rem(z + nz - (s + 1), nz) if way == 0 else lax.rem(z + s + 1, nz)


    half = rows // 2
    wo_rows = r.wo.shape[0]

    def piece(block, c):
        return r.kv.at[c // 2, block, pl.ds((c % 2) * half, half)]

    def own_piece(c):
        return (r.k, r.v)[c // 2].at[pl.ds((c % 2) * half, half)]

    def ring(way, s, c, block, src=None):
        return remote(
            piece(block, c) if src is None else src,
            piece(block, c),
            r.kv_send.at[way, s, c],
            r.kv_recv.at[way, s, c],
            hop_to[way],
        )

    def pair(way, s, c, block):
        return remote(
            piece(block, c),
            piece(block, c),
            r.pair_send.at[way, s, c],
            r.pair_recv.at[way, s, c],
            partner,
        )

    def own_pair(c, block):
        return remote(own_piece(c), piece(block, c), r.own_send.at[c], r.own_recv.at[c], partner)

    def aux_hop(way, s, block, src=None):
        return remote(
            r.aux_all.at[block] if src is None else src,
            r.aux_all.at[block],
            r.aux_send.at[way, s],
            r.aux_recv.at[way, s],
            hop_to[way],
        )

    def wo_copy(o, at):
        return remote(
            r.wo,
            r.wo_all.at[pl.ds(at * wo_rows, wo_rows)],
            r.wo_send.at[o - 1],
            r.wo_recv.at[o - 1],
            across[o - 1],
        )

    for c in range(4):
        for way in (0, 1):
            ring(way, 0, c, sp, own_piece(c)).start()
        own_pair(c, sp).start()
    for o in range(1, nx):
        wo_copy(o, x).start()
    for load in loads:
        load.start()
    named = jnp.concatenate([r.ids[...].astype(F32), r.share[...]], axis=1)
    r.aux_all[z] = named.T
    r.kv[0, sp] = r.k[...]
    r.kv[1, sp] = r.v[...]
    r.wo_all[pl.ds(x * wo_rows, wo_rows), :] = r.wo[...]
    r.acc[...] = jnp.zeros_like(r.acc)
    r.behind[...] = jnp.zeros_like(r.behind)
    r.far[...] = jnp.zeros_like(r.far)
    for way in (0, 1):
        aux_hop(way, 0, z).start()

    span = 2 * KBLK
    above = lax.broadcasted_iota(jnp.int32, (span, span), 0)
    below = lax.broadcasted_iota(jnp.int32, (span, span), 1)
    later_keys = (above > below).astype(F32).astype(BF16)
    to_log2 = HEAD_DIM ** (-0.5) * LOG2E

    def visit(first, blocks, mode):
        q = r.q[...]
        spent_after = jnp.zeros((rows, KBLK), F32) if mode == "far" else r.behind[...]
        total = jnp.zeros((rows, HEAD_DIM), F32)
        for b in reversed(range(blocks * rows // span)):
            block = first + b * span // rows
            at = pl.ds(b * span % rows, span)
            score = (
                lax.dot_general(
                    q,
                    r.kv[0, block, at, :],
                    (((1,), (1,)), ((), ())),
                    preferred_element_type=F32,
                )
                * to_log2
            )
            soft = jnp.maximum(
                score, jnp.log(1.0 + jnp.exp2(jnp.minimum(score, 64.0))) * LOG2E
            )
            if mode == "diagonal":
                key_pos = b * span + lax.broadcasted_iota(jnp.int32, (rows, span), 1)
                query_pos = lax.broadcasted_iota(jnp.int32, (rows, span), 0)
                usable = key_pos < query_pos
                spent = jnp.where(usable, soft, 0.0)
            else:
                spent = soft
            added = jnp.dot(spent.astype(BF16), later_keys, preferred_element_type=F32)
            both = jnp.concatenate([spent_after] * (span // KBLK), axis=1)
            weight = jnp.exp2(((score - soft) - added) - both)
            if mode == "diagonal":
                weight = jnp.where(usable, weight, 0.0)
            spent_after = spent_after + (added[:, :1] + spent[:, :1])
            total = total + jnp.dot(
                weight.astype(BF16), r.kv[1, block, at, :], preferred_element_type=F32
            )
        if mode == "far":
            r.far[...] = r.far[...] * jnp.exp2(-spent_after) + total
        else:
            r.acc[...] = r.acc[...] + total
            r.behind[...] = spent_after

    def work_near(s):
        chip = z - (s + 1)

        @pl.when(chip >= 0)
        def _():
            visit(jnp.maximum(2 * chip, 0), 2, "near")

    def work_far(s):
        chip = z + s + 1 - nz

        @pl.when(chip >= 0)
        def _():
            visit(jnp.maximum(2 * chip, 0), 2, "far")

    def of_pair(way, s):
        return 2 * source(way, s) + 1 - core

    visit(sp, 1, "diagonal")
    other = sp + 1 - 2 * core
    for c in range(4):
        own_pair(c, other).wait_recv()

    @pl.when(core == 1)
    def _():
        visit(other, 1, "near")

    @pl.loop(0, last)
    def _(s):
        for way in (0, 1):
            aux_hop(way, s, source(way, s)).wait_recv()

            @pl.when((s < last - 1) | (way == 0))
            def _():
                aux_hop(way, s + 1, source(way, s)).start()

        for c in range(4):
            for way in (0, 1):
                block = 2 * source(way, s) + core
                ring(way, s, c, block).wait_recv()
                if (c < 2) == (way == 0):
                    ring(way, s + 1, c, block).start()
                else:

                    @pl.when(s < last - 1)
                    def _():
                        ring(way, s + 1, c, block).start()

                pair(way, s, c, block).start()

            if c % 2 == 0:

                @pl.when(s > 0)
                def _():
                    for c2 in range(4):
                        pair(c // 2, s - 1, c2, of_pair(c // 2, s - 1)).wait_recv()
                    (work_near, work_far)[c // 2](s - 1)

    for way in (0, 1):
        for c2 in range(4):
            pair(way, last - 1, c2, of_pair(way, last - 1)).wait_recv()
        (work_near, work_far)[way](last - 1)
    aux_hop(0, last, source(0, last)).wait_recv()
    for c in range(4):
        way = c // 2
        block = 2 * source(way, last) + core
        ring(way, last, c, block).wait_recv()
        pair(way, last, c, block).start()
    for c in range(4):
        way = c // 2
        pair(way, last, c, of_pair(way, last)).wait_recv()
    work_near(last)
    r.att[...] = (r.acc[...] + r.far[...] * jnp.exp2(-r.behind[...])).astype(BF16)


    def head_copy(o, to, at):
        return remote(
            r.att.at[pl.ds(to * tokens, tokens)],
            r.heads.at[at],
            r.head_send.at[o - 1],
            r.head_recv.at[o - 1],
            across[o - 1],
        )

    for o in range(1, nx):
        head_copy(o, lax.rem(x + o, nx), x).start()
    r.heads[x] = r.att[pl.ds(x * tokens, tokens), :]
    for o in range(1, nx):
        wo_copy(o, lax.rem(x + nx - o, nx)).wait_recv()
    for o in range(1, nx):
        head_copy(o, x, lax.rem(x + nx - o, nx)).wait_recv()
    by_token = jnp.concatenate([r.heads[i] for i in range(nx)], axis=1)
    mixed = jnp.dot(by_token, r.wo_all[...], preferred_element_type=F32)
    normed = norm(r.res[...].astype(F32) + mixed, r.gain1[...], r.bias1[...]).astype(BF16)
    r.rows_all[z] = normed


    part = tokens // CHUNKS

    def row_ring(way, s, c, block):
        at = r.rows_all.at[block, pl.ds(c * part, part)]
        return remote(at, at, r.row_send.at[way, s, c], r.row_recv.at[way, s, c], hop_to[way])

    for c in range(CHUNKS):
        for way in (0, 1):
            row_ring(way, 0, c, z).start()
    r.base[...] = r.rows_all[z].astype(F32)

    def chosen(block, side):
        code, _ = slot_codes(r.aux_all[block], z, experts)
        flat = jnp.where(slot_matches(code, side), 1.0, 0.0)
        flat = flat.reshape(experts * 2 * SLOTS, tokens).astype(BF16)
        return jnp.dot(flat, r.rows_all[block], preferred_element_type=F32)

    def outgoing_slot(g):
        return lax.rem(g, 2) if not isinstance(g, int) or g < last else 2

    def slot_copy(o, i, device, g, at, side=None):
        lines = pl.ds(0, 2 * SLOTS) if side is None else pl.ds(side * SLOTS, SLOTS)
        sem = g if side is None else last + side
        return remote(
            r.outgoing.at[i, outgoing_slot(g), lines],
            r.slots.at[at, g, lines],
            r.slot_send.at[o, sem],
            r.slot_recv.at[o, sem],
            device,
        )

    def send_slots(g):
        r.slots[me, g] = r.outgoing[me, outgoing_slot(g)]
        for o, (i, device) in enumerate(peers):
            slot_copy(o, i, device, g, me).start()

    def send_side(found, side):
        lines = slice(side * SLOTS, (side + 1) * SLOTS)
        found = found.astype(BF16).reshape(experts, 2 * SLOTS, width)
        r.outgoing[:, 2, lines] = found[:, lines]
        r.slots[me, last, lines] = r.outgoing[me, 2, lines]
        for o, (i, device) in enumerate(peers):
            slot_copy(o, i, device, last, me, side).start()

    def slots_sent(g):
        for o, (i, device) in enumerate(peers):
            slot_copy(o, i, device, g, i).wait_send()

    def fill(found, g):
        r.outgoing[:, outgoing_slot(g)] = found.astype(BF16).reshape(
            experts, 2 * SLOTS, width
        )
        send_slots(g)

    def back_copy(o, i, device, g, at, side=None):
        lines = pl.ds(0, 2 * SLOTS) if side is None else pl.ds(side * SLOTS, SLOTS)
        return remote(
            r.slots.at[i, g, lines],
            r.back.at[at, g, lines],
            r.back_send.at[o, g],
            r.back_recv.at[o, g],
            device,
        )

    def give_back(g, side=None):
        lines = slice(0, 2 * SLOTS) if side is None else slice(side * SLOTS, (side + 1) * SLOTS)
        r.back[me, g, lines] = r.slots[me, g, lines]
        for o, (i, device) in enumerate(peers):
            back_copy(o, i, device, g, me, side).start()

    def produce(g):
        given = r.slots[:, g].reshape(experts * 2 * SLOTS, width)
        hidden = gated(
            jnp.dot(given, r.gate[0], preferred_element_type=F32),
            jnp.dot(given, r.up[0], preferred_element_type=F32),
        )
        made = jnp.dot(hidden, r.down[0], preferred_element_type=F32)
        r.slots[:, g] = made.astype(BF16).reshape(experts, 2 * SLOTS, width)

    def serve(g):
        for o, (i, device) in enumerate(peers):
            slot_copy(o, i, device, g, i).wait_recv()
        produce(g)


    taken = pl.ds(0, USED)

    def far_send(way, n):
        chip = shift(way, 1) if n < experts else shift(way, 2)
        i = n if n < experts else way * nx + n - experts
        lines = pl.ds(way * SLOTS if n < experts else 0, USED)
        row = way if n < experts else 2
        return remote(
            r.far_out.at[way, n, taken],
            r.slots.at[me, last - 1 if n < experts else last, lines],
            r.far_send.at[way, n],
            r.far_recv.at[row, me],
            member(chip, i),
        )

    def far_arrival(row, i):
        side = row if row < 2 else 0
        here = r.slots.at[i, last - 1 if row < 2 else last, pl.ds(side * SLOTS, USED)]
        return remote(
            r.far_out.at[0, 0, taken], here, r.far_send.at[0, 0], r.far_recv.at[row, i], hop_to[0]
        )

    def far_return(row, i):
        way = row if row < 2 else core
        if row < 2:
            chip, n = shift(1 - row, 1), me
        else:
            chip, n = lax.rem(z + nz - 2 + 4 * core, nz), experts + x
        side = row if row < 2 else 0
        return remote(
            r.slots.at[i, last - 1 if row < 2 else last, pl.ds(side * SLOTS, USED)],
            r.raw_in.at[way, n, taken],
            r.raw_send.at[row, i],
            r.raw_recv.at[way, n],
            member(chip, i),
        )

    def raw_arrival(way, n):
        return remote(
            r.far_out.at[0, 0, taken],
            r.raw_in.at[way, n, taken],
            r.far_send.at[0, 0],
            r.raw_recv.at[way, n],
            hop_to[0],
        )

    def far_codes(way):
        aux = r.aux_all[source(way, last - 2)]
        code_one, share_one = slot_codes(aux, shift(way, 1), experts)
        code_two, share_two = slot_codes(aux, shift(way, 2), experts)
        part_two = slice(way * nx, (way + 1) * nx)
        code = jnp.concatenate([code_one, code_two[part_two]], axis=0)
        share = jnp.concatenate([share_one, share_two[part_two]], axis=0)
        slot = lax.broadcasted_iota(jnp.int32, (experts + nx, SLOTS, tokens), 1).astype(F32)
        return code[:, None, :] == slot, share[:, None, :]

    many = (experts + nx) * SLOTS

    def pass_on(way):
        picks, _ = far_codes(way)
        flat = jnp.where(picks, 1.0, 0.0).reshape(many, tokens).astype(BF16)
        found = jnp.dot(flat, r.rows_all[source(way, last - 2)], preferred_element_type=F32)
        r.far_out[way] = found.astype(BF16).reshape(experts + nx, SLOTS, width)
        for n in reversed(range(experts + nx)):
            far_send(way, n).start()

    for load in loads[:3]:
        load.wait()
    own = r.rows_all[z]
    shared_hidden = gated(
        jnp.dot(own, r.sgate[...], preferred_element_type=F32),
        jnp.dot(own, r.sup[...], preferred_element_type=F32),
    )
    r.base[...] += jnp.dot(shared_hidden, r.sdown[...], preferred_element_type=F32)
    send_side(chosen(z, 1), 1)
    for load in loads[3:]:
        load.wait()

    @pl.loop(0, last - 1)
    def _(s):
        for c in range(CHUNKS):
            for way in (0, 1):
                block = source(way, s)
                row_ring(way, s, c, block).wait_recv()

                @pl.when(s < last - 2)
                def _():
                    row_ring(way, s + 1, c, block).start()

        @pl.when(s == last - 2)
        def _():
            for way in (0, 1):
                pass_on(way)

        @pl.when(s > 1)
        def _():
            slots_sent(s - 2)

        fill(chosen(source(0, s), 0) + chosen(source(1, s), 1), s)

        @pl.when(s > 0)
        def _():
            serve(s - 1)

    serve(last - 2)
    for o, (i, device) in enumerate(peers):
        slot_copy(o, i, device, last, i, 1).wait_recv()
    for i in range(experts):
        far_arrival(2, i).wait_recv()
    produce(last)
    for i in range(experts):
        far_return(2, i).start()
    for row in (0, 1):
        for i in range(experts):
            far_arrival(row, i).wait_recv()
    produce(last - 1)
    for row in (0, 1):
        for i in range(experts):
            far_return(row, i).start()
    for g in (last - 2, last - 3, last - 4):
        give_back(g)
    give_back(last, 1)


    def arrived(g, side=None):
        for o, (i, device) in enumerate(peers):
            back_copy(o, i, device, g, i, side).wait_recv()

    def lines_of(g):
        return r.back[:, g].reshape(experts * 2 * SLOTS, width)

    def weighed(token_chip, side, g):
        code, share = slot_codes(r.aux_all[token_chip], z, experts)
        flat = jnp.where(slot_matches(code, side), share[:, None, :], 0.0)
        flat = flat.reshape(experts * 2 * SLOTS, tokens)
        return jnp.dot(flat.T.astype(BF16), lines_of(g), preferred_element_type=F32)

    def sum_ring(way, s, c):
        at = pl.ds(c * part, part)
        return remote(
            r.sums.at[way, s - 2, at],
            r.held.at[way, s - 2, at],
            r.sum_send.at[way, s - 2, c],
            r.sum_recv.at[way, s - 2, c],
            hop_to[way],
        )

    def part_of(c):
        return slice(c * part, (c + 1) * part)

    def target(way, s):
        return lax.rem(z + hops - s, nz) if way == 0 else lax.rem(z + nz - hops + s, nz)

    def from_far(way):
        picks, share = far_codes(1 - way)
        flat = jnp.where(picks, share, 0.0).reshape(many, tokens)
        lines = r.raw_in[1 - way].reshape(many, width)
        return jnp.dot(flat.T.astype(BF16), lines, preferred_element_type=F32)

    arrived(last - 2)
    near = [weighed(target(way, 2), 1 - way, last - 2) for way in (0, 1)]
    for way in (0, 1):
        for n in range(experts + nx):
            raw_arrival(1 - way, n).wait_recv()
        summed = near[way] + from_far(way)
        r.sums[way, 0] = summed.astype(BF16)
        for c in range(CHUNKS):
            sum_ring(way, 2, c).start()

    @pl.loop(3, hops)
    def _(s):
        g = last - s

        @pl.when(g > 1)
        def _():
            give_back(g - 2)

        arrived(g)
        mine = [weighed(target(way, s), 1 - way, g) for way in (0, 1)]
        for c in range(CHUNKS):
            for way in (0, 1):
                sum_ring(way, s - 1, c).wait_recv()
                summed = mine[way][part_of(c), :] + r.held[way, s - 3, part_of(c), :].astype(F32)
                r.sums[way, s - 2, part_of(c), :] = summed.astype(BF16)
                sum_ring(way, s, c).start()

    arrived(last, 1)
    code, share = slot_codes(r.aux_all[z], z, experts)
    slot = lax.broadcasted_iota(jnp.int32, (experts, SLOTS, tokens), 1).astype(F32)
    flat = jnp.where(code[:, None, :] == slot, share[:, None, :], 0.0)
    r.base[...] += jnp.dot(
        flat.reshape(experts * SLOTS, tokens).T.astype(BF16),
        r.back[:, last, SLOTS:].reshape(experts * SLOTS, width),
        preferred_element_type=F32,
    )
    for c in range(CHUNKS):
        for way in (0, 1):
            sum_ring(way, last, c).wait_recv()
        summed = (
            r.base[part_of(c), :]
            + r.held[0, last - 2, part_of(c), :].astype(F32)
            + r.held[1, last - 2, part_of(c), :].astype(F32)
        )
        r.out[part_of(c), :] = norm(summed, r.gain2[...], r.bias2[...]).astype(r.out.dtype)


    for o in range(1, nx):
        wo_copy(o, x).wait_send()
        head_copy(o, x, x).wait_send()
    for c in range(4):
        own_pair(c, sp).wait_send()

    @pl.loop(0, last)
    def _(s):
        for way in (0, 1):
            aux_hop(way, s, z).wait_send()
            for c in range(4):
                ring(way, s, c, sp).wait_send()
                pair(way, s, c, sp).wait_send()

    aux_hop(0, last, z).wait_send()
    for c in range(4):
        ring(c // 2, last, c, sp).wait_send()
        pair(c // 2, last, c, sp).wait_send()

    @pl.loop(0, last - 1)
    def _(s):
        for way in (0, 1):
            for c in range(CHUNKS):
                row_ring(way, s, c, z).wait_send()
                sum_ring(way, s + 2, c).wait_send()

    for way in (0, 1):
        for n in range(experts + nx):
            far_send(way, n).wait_send()
    for row in range(3):
        for i in range(experts):
            far_return(row, i).wait_send()
    slots_sent(last - 3)
    slots_sent(last - 2)
    for o, (i, device) in enumerate(peers):
        slot_copy(o, i, device, last, i, 1).wait_send()
        back_copy(o, i, device, last, i, 1).wait_send()

    @pl.loop(0, last - 1)
    def _(g):
        for o, (i, device) in enumerate(peers):
            back_copy(o, i, device, g, i).wait_send()


REFS = (
    "q",
    "k",
    "v",
    "wo",
    "ids",
    "share",
    "res",
    "gain1",
    "bias1",
    "gain2",
    "bias2",
    "gate_hbm",
    "up_hbm",
    "down_hbm",
    "sgate_hbm",
    "sup_hbm",
    "sdown_hbm",
    "out",
    "kv",
    "acc",
    "behind",
    "far",
    "aux_all",
    "wo_all",
    "att",
    "heads",
    "rows_all",
    "base",
    "outgoing",
    "slots",
    "back",
    "gate",
    "up",
    "down",
    "sgate",
    "sup",
    "sdown",
    "far_out",
    "raw_in",
    "sums",
    "held",
    "load_sem",
    "kv_send",
    "kv_recv",
    "pair_send",
    "pair_recv",
    "own_send",
    "own_recv",
    "aux_send",
    "aux_recv",
    "wo_send",
    "wo_recv",
    "head_send",
    "head_recv",
    "row_send",
    "row_recv",
    "slot_send",
    "slot_recv",
    "back_send",
    "back_recv",
    "far_send",
    "far_recv",
    "raw_send",
    "raw_recv",
    "sum_send",
    "sum_recv",
)


def layer(nz, nx, q, k, v, wo, ids, share, res, norms, weights, shared):
    rows, head = q.shape
    tokens, width = res.shape
    hops = nz // 2
    experts = 2 * nx
    whole = pl.BlockSpec(memory_space=pltpu.VMEM)
    anywhere = pl.BlockSpec(memory_space=pl.ANY)
    dma = pltpu.SemaphoreType.DMA
    slot_shape = (experts, hops, 2 * SLOTS, width)
    return pl.pallas_call(
        functools.partial(layer_kernel, nz, nx),
        name="layer",
        out_shape=jax.ShapeDtypeStruct((tokens, width), BF16),
        in_specs=[whole] * 11 + [anywhere] * 6,
        out_specs=whole,
        scratch_shapes=[
            pltpu.VMEM((2, 2 * nz, rows, head), BF16),
            pltpu.VMEM((rows, head), F32),
            pltpu.VMEM((rows, KBLK), F32),
            pltpu.VMEM((rows, head), F32),
            pltpu.VMEM((nz, 2 * ids.shape[1], tokens), F32),
            pltpu.VMEM((nx * wo.shape[0], width), BF16),
            pltpu.VMEM((rows, head), BF16),
            pltpu.VMEM((nx, tokens, head), BF16),
            pltpu.VMEM((nz, tokens, width), BF16),
            pltpu.VMEM((tokens, width), F32),
            pltpu.VMEM((experts, 3, 2 * SLOTS, width), BF16),
            pltpu.VMEM(slot_shape, BF16),
            pltpu.VMEM(slot_shape, BF16),
            *[pltpu.VMEM(w.shape, BF16) for w in (*weights, *shared)],
            pltpu.VMEM((2, experts + nx, SLOTS, width), BF16),
            pltpu.VMEM((2, experts + nx, SLOTS, width), BF16),
            pltpu.VMEM((2, hops - 2, tokens, width), BF16),
            pltpu.VMEM((2, hops - 2, tokens, width), BF16),
            dma((6,)),
            dma((2, hops, 4)),
            dma((2, hops, 4)),
            dma((2, hops, 4)),
            dma((2, hops, 4)),
            dma((4,)),
            dma((4,)),
            dma((2, hops)),
            dma((2, hops)),
            dma((nx - 1,)),
            dma((nx - 1,)),
            dma((nx - 1,)),
            dma((nx - 1,)),
            dma((2, hops - 2, CHUNKS)),
            dma((2, hops - 2, CHUNKS)),
            dma((experts - 1, hops + 1)),
            dma((experts - 1, hops + 1)),
            dma((experts - 1, hops)),
            dma((experts - 1, hops)),
            dma((2, experts + nx)),
            dma((3, experts)),
            dma((3, experts)),
            dma((2, experts + nx)),
            dma((2, hops - 2, CHUNKS)),
            dma((2, hops - 2, CHUNKS)),
        ],
        compiler_params=pltpu.CompilerParams(
            collective_id=0, has_side_effects=True, vmem_limit_bytes=67_000_000
        ),
        cost_estimate=pl.CostEstimate(flops=1 << 34, bytes_accessed=1 << 24, transcendentals=0),
    )(q, k, v, wo, ids, share, res, *norms, *weights, *shared)


def local(
    query_rows,
    key_rows,
    value_rows,
    residual,
    output_weight,
    first_gain,
    first_bias,
    expert_ids,
    expert_share,
    gate_weight,
    up_weight,
    down_weight,
    shared_gate,
    shared_up,
    shared_down,
    second_gain,
    second_bias,
):
    nz = lax.axis_size("sp") // 2
    nx = lax.axis_size("tp")
    norms = [a[None, :] for a in (first_gain, first_bias, second_gain, second_bias)]
    return layer(
        nz,
        nx,
        query_rows,
        key_rows,
        value_rows,
        output_weight,
        expert_ids,
        expert_share,
        residual,
        norms,
        (gate_weight, up_weight, down_weight),
        (shared_gate, shared_up, shared_down),
    )


def solution(mesh):
    return jax.shard_map(
        local,
        mesh=mesh,
        in_specs=(
            P(("grp", "sp"), "tp"),
            P(("grp", "sp"), "tp"),
            P(("grp", "sp"), "tp"),
            P(("grp", "sp", "tp"), None),
            P("tp", None),
            P(),
            P(),
            P(("grp", "sp", "tp"), None),
            P(("grp", "sp", "tp"), None),
            P(("sp", "tp"), None, None),
            P(("sp", "tp"), None, None),
            P(("sp", "tp"), None, None),
            P(),
            P(),
            P(),
            P(),
            P(),
        ),
        out_specs=P(("grp", "sp", "tp"), None),
        check_vma=False,
    )
```

```python
import functools

import jax
import jax.numpy as jnp
from jax import lax
from jax.experimental import pallas as pl
from jax.experimental.pallas import tpu as pltpu
from jax.sharding import PartitionSpec as P

HEAD_DIM = 128
KBLK = 128
NORM_EPS = 1e-05
LOG2E = 1.4426950408889634
MESH = pl.DeviceIdType.MESH
SLOTS = 8
USED = 6
BF16 = jnp.bfloat16
F32 = jnp.float32


def at_sp(sp):
    return {"sp": sp}


def place():
    sp = lax.axis_index("sp")
    return sp, sp // 2, sp % 2, lax.axis_index("tp")


def greet(devices):
    barrier = pltpu.get_barrier_semaphore()
    for device in devices:
        pl.semaphore_signal(barrier, inc=1, device_id=device, device_id_type=MESH)
    pl.semaphore_wait(barrier, len(devices))


def remote(src, dst, send_sem, recv_sem, device):
    return pltpu.make_async_remote_copy(
        src_ref=src,
        dst_ref=dst,
        send_sem=send_sem,
        recv_sem=recv_sem,
        device_id=device,
        device_id_type=MESH,
    )


def slot_codes(aux, z, experts):
    width = aux.shape[1]
    picks = aux.shape[0] // 2
    number = (z * experts + lax.broadcasted_iota(jnp.int32, (experts, width), 0)).astype(F32)
    named = jnp.zeros((experts, width), F32)
    share = jnp.zeros((experts, width), F32)
    for k in range(picks):
        hit = aux[k : k + 1, :] == number
        named = named + jnp.where(hit, 1.0, 0.0)
        share = share + jnp.where(hit, aux[picks + k : picks + k + 1, :], 0.0)
    earlier = lax.broadcasted_iota(jnp.int32, (width, width), 0)
    later = lax.broadcasted_iota(jnp.int32, (width, width), 1)
    before = (earlier < later).astype(F32).astype(BF16)
    rank = jnp.dot(named.astype(BF16), before, preferred_element_type=F32)
    return jnp.where(named > 0.0, rank, -1000.0), share


def slot_matches(code, side):
    experts, width = code.shape
    slot = lax.broadcasted_iota(jnp.int32, (experts, 2 * SLOTS, width), 1).astype(F32)
    return (code[:, None, :] + float(side * SLOTS)) == slot


def norm(summed, gains, offset):
    average = jnp.mean(summed, axis=-1, keepdims=True)
    centred = summed - average
    spread = jnp.mean(centred * centred, axis=-1, keepdims=True)
    return centred * lax.rsqrt(spread + NORM_EPS) * gains + offset


def gated(gate_act, up_act):
    return (gate_act / (1.0 + jnp.exp(-gate_act)) * up_act).astype(BF16)


CHUNKS = 4


def group_peers(nx, core, x, z):
    me = core * nx + x
    peers = []
    for o in range(1, 2 * nx):
        i = lax.rem(me + o, 2 * nx)
        peers.append((i, {"sp": 2 * z + i // nx, "tp": lax.rem(i, nx)}))
    return me, peers


class Names:
    pass


def layer_kernel(nz, nx, *refs):
    sp, z, core, x = place()
    nsp = 2 * nz
    r = Names()
    for name, ref in zip(REFS, refs, strict=True):
        setattr(r, name, ref)
    hop_to = (at_sp(lax.rem(sp + 2, nsp)), at_sp(lax.rem(sp + nsp - 2, nsp)))
    partner = at_sp(sp + 1 - 2 * core)
    across = [{"tp": lax.rem(x + o, nx)} for o in range(1, nx)]
    me, peers = group_peers(nx, core, x, z)

    def shift(way, by):
        return lax.rem(z + by, nz) if way == 0 else lax.rem(z + nz - by, nz)

    def member(chip, i):
        return {"sp": 2 * chip + i // nx, "tp": i % nx}

    heads_at = pl.ds(x * r.wo_hbm.shape[0], r.wo_hbm.shape[0])
    first_loads = [
        pltpu.make_async_copy(src, dst, r.first_sem.at[n])
        for n, (src, dst) in enumerate(
            (
                (r.k_hbm, r.kv.at[0, sp]),
                (r.v_hbm, r.kv.at[1, sp]),
                (r.q_hbm, r.q),
                (r.wo_hbm, r.wo_all.at[heads_at]),
                (r.res_hbm, r.res),
            )
        )
    ]
    for load in first_loads:
        load.start()
    r.raw_in[...] = jnp.zeros_like(r.raw_in)
    greet(
        [device for _, device in peers]
        + [
            member(shift(way, by), i)
            for by in (1, 2)
            for way in (0, 1)
            for i in range(2 * nx)
        ]
    )

    hops = nz // 2
    last = hops - 1
    experts = 2 * nx
    tokens, width = r.res.shape
    rows = r.q.shape[0]

    loads = [
        pltpu.make_async_copy(src, dst, r.load_sem.at[n])
        for n, (src, dst) in enumerate(
            (
                (r.sgate_hbm, r.sgate),
                (r.sup_hbm, r.sup),
                (r.sdown_hbm, r.sdown),
                (r.gate_hbm, r.gate),
                (r.up_hbm, r.up),
                (r.down_hbm, r.down),
            )
        )
    ]

    def source(way, s):
        return lax.rem(z + nz - (s + 1), nz) if way == 0 else lax.rem(z + s + 1, nz)


    half = rows // 2
    wo_rows = r.wo_hbm.shape[0]

    def piece(block, c):
        return r.kv.at[c // 2, block, pl.ds((c % 2) * half, half)]

    def ring(way, s, c, block):
        return remote(
            piece(block, c),
            piece(block, c),
            r.kv_send.at[way, s, c],
            r.kv_recv.at[way, s, c],
            hop_to[way],
        )

    def pair(way, s, c, block):
        return remote(
            piece(block, c),
            piece(block, c),
            r.pair_send.at[way, s, c],
            r.pair_recv.at[way, s, c],
            partner,
        )

    def own_pair(c, block):
        return remote(piece(block, c), piece(block, c), r.own_send.at[c], r.own_recv.at[c], partner)

    def aux_hop(way, s, block, src=None):
        return remote(
            r.aux_all.at[block] if src is None else src,
            r.aux_all.at[block],
            r.aux_send.at[way, s],
            r.aux_recv.at[way, s],
            hop_to[way],
        )

    def wo_copy(o, at):
        return remote(
            r.wo_all.at[pl.ds(at * wo_rows, wo_rows)],
            r.wo_all.at[pl.ds(at * wo_rows, wo_rows)],
            r.wo_send.at[o - 1],
            r.wo_recv.at[o - 1],
            across[o - 1],
        )

    for c in range(4):
        if c % 2 == 0:
            first_loads[c // 2].wait()
        for way in (0, 1):
            ring(way, 0, c, sp).start()
        own_pair(c, sp).start()
    for load in first_loads[2:]:
        load.wait()
    for o in range(1, nx):
        wo_copy(o, x).start()
    for load in loads:
        load.start()
    r.aux_all[z] = jnp.concatenate([r.ids[...].astype(F32), r.share[...]], axis=0)
    r.acc[...] = jnp.zeros_like(r.acc)
    r.behind[...] = jnp.zeros_like(r.behind)
    r.far[...] = jnp.zeros_like(r.far)
    for way in (0, 1):
        aux_hop(way, 0, z).start()

    span = 2 * KBLK
    above = lax.broadcasted_iota(jnp.int32, (span, span), 0)
    below = lax.broadcasted_iota(jnp.int32, (span, span), 1)
    later_keys = (above > below).astype(F32).astype(BF16)
    to_log2 = HEAD_DIM ** (-0.5) * LOG2E

    def visit(first, blocks, mode):
        q = r.q[...]
        spent_after = jnp.zeros((rows, KBLK), F32) if mode == "far" else r.behind[...]
        total = jnp.zeros((rows, HEAD_DIM), F32)
        for b in reversed(range(blocks * rows // span)):
            block = first + b * span // rows
            at = pl.ds(b * span % rows, span)
            score = (
                lax.dot_general(
                    q,
                    r.kv[0, block, at, :],
                    (((1,), (1,)), ((), ())),
                    preferred_element_type=F32,
                )
                * to_log2
            )
            soft = jnp.maximum(
                score, jnp.log(1.0 + jnp.exp2(jnp.minimum(score, 64.0))) * LOG2E
            )
            if mode == "diagonal":
                key_pos = b * span + lax.broadcasted_iota(jnp.int32, (rows, span), 1)
                query_pos = lax.broadcasted_iota(jnp.int32, (rows, span), 0)
                usable = key_pos < query_pos
                spent = jnp.where(usable, soft, 0.0)
            else:
                spent = soft
            added = jnp.dot(spent.astype(BF16), later_keys, preferred_element_type=F32)
            both = jnp.concatenate([spent_after] * (span // KBLK), axis=1)
            weight = jnp.exp2(((score - soft) - added) - both)
            if mode == "diagonal":
                weight = jnp.where(usable, weight, 0.0)
            spent_after = spent_after + (added[:, :1] + spent[:, :1])
            total = total + jnp.dot(
                weight.astype(BF16), r.kv[1, block, at, :], preferred_element_type=F32
            )
        if mode == "far":
            r.far[...] = r.far[...] * jnp.exp2(-spent_after) + total
        else:
            r.acc[...] = r.acc[...] + total
            r.behind[...] = spent_after

    def work_near(s):
        chip = z - (s + 1)

        @pl.when(chip >= 0)
        def _():
            visit(jnp.maximum(2 * chip, 0), 2, "near")

    def work_far(s):
        chip = z + s + 1 - nz

        @pl.when(chip >= 0)
        def _():
            visit(jnp.maximum(2 * chip, 0), 2, "far")

    def of_pair(way, s):
        return 2 * source(way, s) + 1 - core

    visit(sp, 1, "diagonal")
    other = sp + 1 - 2 * core
    for c in range(4):
        own_pair(c, other).wait_recv()

    @pl.when(core == 1)
    def _():
        visit(other, 1, "near")

    @pl.loop(0, last)
    def _(s):
        for way in (0, 1):
            aux_hop(way, s, source(way, s)).wait_recv()

            @pl.when((s < last - 1) | (way == 0))
            def _():
                aux_hop(way, s + 1, source(way, s)).start()

        for c in range(4):
            for way in (0, 1):
                block = 2 * source(way, s) + core
                ring(way, s, c, block).wait_recv()
                if (c < 2) == (way == 0):
                    ring(way, s + 1, c, block).start()
                else:

                    @pl.when(s < last - 1)
                    def _():
                        ring(way, s + 1, c, block).start()

                pair(way, s, c, block).start()

            if c % 2 == 0:

                @pl.when(s > 0)
                def _():
                    for c2 in range(4):
                        pair(c // 2, s - 1, c2, of_pair(c // 2, s - 1)).wait_recv()
                    (work_near, work_far)[c // 2](s - 1)

    for way in (0, 1):
        for c2 in range(4):
            pair(way, last - 1, c2, of_pair(way, last - 1)).wait_recv()
        (work_near, work_far)[way](last - 1)
    aux_hop(0, last, source(0, last)).wait_recv()
    for c in range(4):
        way = c // 2
        block = 2 * source(way, last) + core
        ring(way, last, c, block).wait_recv()
        pair(way, last, c, block).start()
    for c in range(4):
        way = c // 2
        pair(way, last, c, of_pair(way, last)).wait_recv()
    work_near(last)
    r.att[...] = (r.acc[...] + r.far[...] * jnp.exp2(-r.behind[...])).astype(BF16)


    def head_copy(o, to, at):
        return remote(
            r.att.at[pl.ds(to * tokens, tokens)],
            r.heads.at[at],
            r.head_send.at[o - 1],
            r.head_recv.at[o - 1],
            across[o - 1],
        )

    for o in range(1, nx):
        head_copy(o, lax.rem(x + o, nx), x).start()
    r.heads[x] = r.att[pl.ds(x * tokens, tokens), :]
    for o in range(1, nx):
        wo_copy(o, lax.rem(x + nx - o, nx)).wait_recv()
    for o in range(1, nx):
        head_copy(o, x, lax.rem(x + nx - o, nx)).wait_recv()
    by_token = jnp.concatenate([r.heads[i] for i in range(nx)], axis=1)
    mixed = jnp.dot(by_token, r.wo_all[...], preferred_element_type=F32)
    normed = norm(r.res[...].astype(F32) + mixed, r.gain1[...], r.bias1[...]).astype(BF16)
    r.rows_all[z] = normed


    part = tokens // CHUNKS

    def row_ring(way, s, c, block):
        at = r.rows_all.at[block, pl.ds(c * part, part)]
        return remote(at, at, r.row_send.at[way, s, c], r.row_recv.at[way, s, c], hop_to[way])

    for c in range(CHUNKS):
        for way in (0, 1):
            row_ring(way, 0, c, z).start()
    r.base[...] = r.rows_all[z].astype(F32)

    def chosen(block, side):
        code, _ = slot_codes(r.aux_all[block], z, experts)
        flat = jnp.where(slot_matches(code, side), 1.0, 0.0)
        flat = flat.reshape(experts * 2 * SLOTS, tokens).astype(BF16)
        return jnp.dot(flat, r.rows_all[block], preferred_element_type=F32)

    def outgoing_slot(g):
        return lax.rem(g, 2) if not isinstance(g, int) or g < last else 2

    def slot_copy(o, i, device, g, at, side=None):
        lines = pl.ds(0, 2 * SLOTS) if side is None else pl.ds(side * SLOTS, SLOTS)
        sem = g if side is None else last + side
        return remote(
            r.outgoing.at[i, outgoing_slot(g), lines],
            r.slots.at[at, g, lines],
            r.slot_send.at[o, sem],
            r.slot_recv.at[o, sem],
            device,
        )

    def send_slots(g):
        r.slots[me, g] = r.outgoing[me, outgoing_slot(g)]
        for o, (i, device) in enumerate(peers):
            slot_copy(o, i, device, g, me).start()

    def send_side(found, side):
        lines = slice(side * SLOTS, (side + 1) * SLOTS)
        found = found.astype(BF16).reshape(experts, 2 * SLOTS, width)
        r.outgoing[:, 2, lines] = found[:, lines]
        r.slots[me, last, lines] = r.outgoing[me, 2, lines]
        for o, (i, device) in enumerate(peers):
            slot_copy(o, i, device, last, me, side).start()

    def slots_sent(g):
        for o, (i, device) in enumerate(peers):
            slot_copy(o, i, device, g, i).wait_send()

    def fill(found, g):
        r.outgoing[:, outgoing_slot(g)] = found.astype(BF16).reshape(
            experts, 2 * SLOTS, width
        )
        send_slots(g)

    def back_copy(o, i, device, g, at, side=None):
        lines = pl.ds(0, 2 * SLOTS) if side is None else pl.ds(side * SLOTS, SLOTS)
        return remote(
            r.slots.at[i, g, lines],
            r.back.at[at, g, lines],
            r.back_send.at[o, g],
            r.back_recv.at[o, g],
            device,
        )

    def give_back(g, side=None):
        lines = slice(0, 2 * SLOTS) if side is None else slice(side * SLOTS, (side + 1) * SLOTS)
        r.back[me, g, lines] = r.slots[me, g, lines]
        for o, (i, device) in enumerate(peers):
            back_copy(o, i, device, g, me, side).start()

    def produce(g):
        given = r.slots[:, g].reshape(experts * 2 * SLOTS, width)
        hidden = gated(
            jnp.dot(given, r.gate[0], preferred_element_type=F32),
            jnp.dot(given, r.up[0], preferred_element_type=F32),
        )
        made = jnp.dot(hidden, r.down[0], preferred_element_type=F32)
        r.slots[:, g] = made.astype(BF16).reshape(experts, 2 * SLOTS, width)

    def serve(g):
        for o, (i, device) in enumerate(peers):
            slot_copy(o, i, device, g, i).wait_recv()
        produce(g)


    taken = pl.ds(0, USED)

    def far_send(way, n):
        chip = shift(way, 1) if n < experts else shift(way, 2)
        i = n if n < experts else way * nx + n - experts
        lines = pl.ds(way * SLOTS if n < experts else 0, USED)
        row = way if n < experts else 2
        return remote(
            r.far_out.at[way, n, taken],
            r.slots.at[me, last - 1 if n < experts else last, lines],
            r.far_send.at[way, n],
            r.far_recv.at[row, me],
            member(chip, i),
        )

    def far_arrival(row, i):
        side = row if row < 2 else 0
        here = r.slots.at[i, last - 1 if row < 2 else last, pl.ds(side * SLOTS, USED)]
        return remote(
            r.far_out.at[0, 0, taken], here, r.far_send.at[0, 0], r.far_recv.at[row, i], hop_to[0]
        )

    def far_return(row, i):
        way = row if row < 2 else core
        if row < 2:
            chip, n = shift(1 - row, 1), me
        else:
            chip, n = lax.rem(z + nz - 2 + 4 * core, nz), experts + x
        side = row if row < 2 else 0
        return remote(
            r.slots.at[i, last - 1 if row < 2 else last, pl.ds(side * SLOTS, USED)],
            r.raw_in.at[way, n, taken],
            r.raw_send.at[row, i],
            r.raw_recv.at[way, n],
            member(chip, i),
        )

    def raw_arrival(way, n):
        return remote(
            r.far_out.at[0, 0, taken],
            r.raw_in.at[way, n, taken],
            r.far_send.at[0, 0],
            r.raw_recv.at[way, n],
            hop_to[0],
        )

    def far_codes(way):
        aux = r.aux_all[source(way, last - 2)]
        code_one, share_one = slot_codes(aux, shift(way, 1), experts)
        code_two, share_two = slot_codes(aux, shift(way, 2), experts)
        part_two = slice(way * nx, (way + 1) * nx)
        code = jnp.concatenate([code_one, code_two[part_two]], axis=0)
        share = jnp.concatenate([share_one, share_two[part_two]], axis=0)
        slot = lax.broadcasted_iota(jnp.int32, (experts + nx, SLOTS, tokens), 1).astype(F32)
        return code[:, None, :] == slot, share[:, None, :]

    many = (experts + nx) * SLOTS

    def pass_on(way):
        picks, _ = far_codes(way)
        flat = jnp.where(picks, 1.0, 0.0).reshape(many, tokens).astype(BF16)
        found = jnp.dot(flat, r.rows_all[source(way, last - 2)], preferred_element_type=F32)
        r.far_out[way] = found.astype(BF16).reshape(experts + nx, SLOTS, width)
        for n in reversed(range(experts + nx)):
            far_send(way, n).start()

    for load in loads[:3]:
        load.wait()
    own = r.rows_all[z]
    shared_hidden = gated(
        jnp.dot(own, r.sgate[...], preferred_element_type=F32),
        jnp.dot(own, r.sup[...], preferred_element_type=F32),
    )
    r.base[...] += jnp.dot(shared_hidden, r.sdown[...], preferred_element_type=F32)
    send_side(chosen(z, 1), 1)
    for load in loads[3:]:
        load.wait()

    @pl.loop(0, last - 1)
    def _(s):
        for c in range(CHUNKS):
            for way in (0, 1):
                block = source(way, s)
                row_ring(way, s, c, block).wait_recv()

                @pl.when(s < last - 2)
                def _():
                    row_ring(way, s + 1, c, block).start()

        @pl.when(s == last - 2)
        def _():
            for way in (0, 1):
                pass_on(way)

        @pl.when(s > 1)
        def _():
            slots_sent(s - 2)

        fill(chosen(source(0, s), 0) + chosen(source(1, s), 1), s)

        @pl.when(s > 0)
        def _():
            serve(s - 1)

    serve(last - 2)
    for o, (i, device) in enumerate(peers):
        slot_copy(o, i, device, last, i, 1).wait_recv()
    for i in range(experts):
        far_arrival(2, i).wait_recv()
    produce(last)
    for i in range(experts):
        far_return(2, i).start()
    for row in (0, 1):
        for i in range(experts):
            far_arrival(row, i).wait_recv()
    produce(last - 1)
    for row in (0, 1):
        for i in range(experts):
            far_return(row, i).start()
    for g in (last - 2, last - 3, last - 4):
        give_back(g)
    give_back(last, 1)


    def arrived(g, side=None):
        for o, (i, device) in enumerate(peers):
            back_copy(o, i, device, g, i, side).wait_recv()

    def lines_of(g):
        return r.back[:, g].reshape(experts * 2 * SLOTS, width)

    def weighed(token_chip, side, g):
        code, share = slot_codes(r.aux_all[token_chip], z, experts)
        flat = jnp.where(slot_matches(code, side), share[:, None, :], 0.0)
        flat = flat.reshape(experts * 2 * SLOTS, tokens)
        return jnp.dot(flat.T.astype(BF16), lines_of(g), preferred_element_type=F32)

    def sum_ring(way, s, c):
        at = pl.ds(c * part, part)
        return remote(
            r.sums.at[way, s - 2, at],
            r.held.at[way, s - 2, at],
            r.sum_send.at[way, s - 2, c],
            r.sum_recv.at[way, s - 2, c],
            hop_to[way],
        )

    def part_of(c):
        return slice(c * part, (c + 1) * part)

    def target(way, s):
        return lax.rem(z + hops - s, nz) if way == 0 else lax.rem(z + nz - hops + s, nz)

    def from_far(way):
        picks, share = far_codes(1 - way)
        flat = jnp.where(picks, share, 0.0).reshape(many, tokens)
        lines = r.raw_in[1 - way].reshape(many, width)
        return jnp.dot(flat.T.astype(BF16), lines, preferred_element_type=F32)

    arrived(last - 2)
    near = [weighed(target(way, 2), 1 - way, last - 2) for way in (0, 1)]
    for way in (0, 1):
        for n in range(experts + nx):
            raw_arrival(1 - way, n).wait_recv()
        summed = near[way] + from_far(way)
        r.sums[way, 0] = summed.astype(BF16)
        for c in range(CHUNKS):
            sum_ring(way, 2, c).start()

    @pl.loop(3, hops)
    def _(s):
        g = last - s

        @pl.when(g > 1)
        def _():
            give_back(g - 2)

        arrived(g)
        mine = [weighed(target(way, s), 1 - way, g) for way in (0, 1)]
        for c in range(CHUNKS):
            for way in (0, 1):
                sum_ring(way, s - 1, c).wait_recv()
                summed = mine[way][part_of(c), :] + r.held[way, s - 3, part_of(c), :].astype(F32)
                r.sums[way, s - 2, part_of(c), :] = summed.astype(BF16)
                sum_ring(way, s, c).start()

    arrived(last, 1)
    code, share = slot_codes(r.aux_all[z], z, experts)
    slot = lax.broadcasted_iota(jnp.int32, (experts, SLOTS, tokens), 1).astype(F32)
    flat = jnp.where(code[:, None, :] == slot, share[:, None, :], 0.0)
    r.base[...] += jnp.dot(
        flat.reshape(experts * SLOTS, tokens).T.astype(BF16),
        r.back[:, last, SLOTS:].reshape(experts * SLOTS, width),
        preferred_element_type=F32,
    )
    for c in range(CHUNKS):
        for way in (0, 1):
            sum_ring(way, last, c).wait_recv()
        summed = (
            r.base[part_of(c), :]
            + r.held[0, last - 2, part_of(c), :].astype(F32)
            + r.held[1, last - 2, part_of(c), :].astype(F32)
        )
        r.out[part_of(c), :] = norm(summed, r.gain2[...], r.bias2[...]).astype(r.out.dtype)


    for o in range(1, nx):
        wo_copy(o, x).wait_send()
        head_copy(o, x, x).wait_send()
    for c in range(4):
        own_pair(c, sp).wait_send()

    @pl.loop(0, last)
    def _(s):
        for way in (0, 1):
            aux_hop(way, s, z).wait_send()
            for c in range(4):
                ring(way, s, c, sp).wait_send()
                pair(way, s, c, sp).wait_send()

    aux_hop(0, last, z).wait_send()
    for c in range(4):
        ring(c // 2, last, c, sp).wait_send()
        pair(c // 2, last, c, sp).wait_send()

    @pl.loop(0, last - 1)
    def _(s):
        for way in (0, 1):
            for c in range(CHUNKS):
                row_ring(way, s, c, z).wait_send()
                sum_ring(way, s + 2, c).wait_send()

    for way in (0, 1):
        for n in range(experts + nx):
            far_send(way, n).wait_send()
    for row in range(3):
        for i in range(experts):
            far_return(row, i).wait_send()
    slots_sent(last - 3)
    slots_sent(last - 2)
    for o, (i, device) in enumerate(peers):
        slot_copy(o, i, device, last, i, 1).wait_send()
        back_copy(o, i, device, last, i, 1).wait_send()

    @pl.loop(0, last - 1)
    def _(g):
        for o, (i, device) in enumerate(peers):
            back_copy(o, i, device, g, i).wait_send()


REFS = (
    "q_hbm",
    "k_hbm",
    "v_hbm",
    "wo_hbm",
    "ids",
    "share",
    "res_hbm",
    "gain1",
    "bias1",
    "gain2",
    "bias2",
    "gate_hbm",
    "up_hbm",
    "down_hbm",
    "sgate_hbm",
    "sup_hbm",
    "sdown_hbm",
    "out",
    "q",
    "res",
    "kv",
    "acc",
    "behind",
    "far",
    "aux_all",
    "wo_all",
    "att",
    "heads",
    "rows_all",
    "base",
    "outgoing",
    "slots",
    "back",
    "gate",
    "up",
    "down",
    "sgate",
    "sup",
    "sdown",
    "far_out",
    "raw_in",
    "sums",
    "held",
    "first_sem",
    "load_sem",
    "kv_send",
    "kv_recv",
    "pair_send",
    "pair_recv",
    "own_send",
    "own_recv",
    "aux_send",
    "aux_recv",
    "wo_send",
    "wo_recv",
    "head_send",
    "head_recv",
    "row_send",
    "row_recv",
    "slot_send",
    "slot_recv",
    "back_send",
    "back_recv",
    "far_send",
    "far_recv",
    "raw_send",
    "raw_recv",
    "sum_send",
    "sum_recv",
)


def layer(nz, nx, q, k, v, wo, ids, share, res, norms, weights, shared):
    rows, head = q.shape
    tokens, width = res.shape
    hops = nz // 2
    experts = 2 * nx
    whole = pl.BlockSpec(memory_space=pltpu.VMEM)
    anywhere = pl.BlockSpec(memory_space=pl.ANY)
    dma = pltpu.SemaphoreType.DMA
    slot_shape = (experts, hops, 2 * SLOTS, width)
    return pl.pallas_call(
        functools.partial(layer_kernel, nz, nx),
        name="layer",
        out_shape=jax.ShapeDtypeStruct((tokens, width), BF16),
        in_specs=[anywhere] * 4 + [whole] * 2 + [anywhere] + [whole] * 4 + [anywhere] * 6,
        out_specs=whole,
        scratch_shapes=[
            pltpu.VMEM((rows, head), BF16),
            pltpu.VMEM((tokens, width), BF16),
            pltpu.VMEM((2, 2 * nz, rows, head), BF16),
            pltpu.VMEM((rows, head), F32),
            pltpu.VMEM((rows, KBLK), F32),
            pltpu.VMEM((rows, head), F32),
            pltpu.VMEM((nz, 2 * ids.shape[0], tokens), F32),
            pltpu.VMEM((nx * wo.shape[0], width), BF16),
            pltpu.VMEM((rows, head), BF16),
            pltpu.VMEM((nx, tokens, head), BF16),
            pltpu.VMEM((nz, tokens, width), BF16),
            pltpu.VMEM((tokens, width), F32),
            pltpu.VMEM((experts, 3, 2 * SLOTS, width), BF16),
            pltpu.VMEM(slot_shape, BF16),
            pltpu.VMEM(slot_shape, BF16),
            *[pltpu.VMEM(w.shape, BF16) for w in (*weights, *shared)],
            pltpu.VMEM((2, experts + nx, SLOTS, width), BF16),
            pltpu.VMEM((2, experts + nx, SLOTS, width), BF16),
            pltpu.VMEM((2, hops - 2, tokens, width), BF16),
            pltpu.VMEM((2, hops - 2, tokens, width), BF16),
            dma((5,)),
            dma((6,)),
            dma((2, hops, 4)),
            dma((2, hops, 4)),
            dma((2, hops, 4)),
            dma((2, hops, 4)),
            dma((4,)),
            dma((4,)),
            dma((2, hops)),
            dma((2, hops)),
            dma((nx - 1,)),
            dma((nx - 1,)),
            dma((nx - 1,)),
            dma((nx - 1,)),
            dma((2, hops - 2, CHUNKS)),
            dma((2, hops - 2, CHUNKS)),
            dma((experts - 1, hops + 1)),
            dma((experts - 1, hops + 1)),
            dma((experts - 1, hops)),
            dma((experts - 1, hops)),
            dma((2, experts + nx)),
            dma((3, experts)),
            dma((3, experts)),
            dma((2, experts + nx)),
            dma((2, hops - 2, CHUNKS)),
            dma((2, hops - 2, CHUNKS)),
        ],
        compiler_params=pltpu.CompilerParams(
            collective_id=0, has_side_effects=True, vmem_limit_bytes=67_000_000
        ),
        cost_estimate=pl.CostEstimate(flops=1 << 34, bytes_accessed=1 << 24, transcendentals=0),
    )(q, k, v, wo, ids, share, res, *norms, *weights, *shared)


def local(
    query_rows,
    key_rows,
    value_rows,
    residual,
    output_weight,
    first_gain,
    first_bias,
    expert_ids,
    expert_share,
    gate_weight,
    up_weight,
    down_weight,
    shared_gate,
    shared_up,
    shared_down,
    second_gain,
    second_bias,
):
    nz = lax.axis_size("sp") // 2
    nx = lax.axis_size("tp")
    norms = [a[None, :] for a in (first_gain, first_bias, second_gain, second_bias)]
    return layer(
        nz,
        nx,
        query_rows,
        key_rows,
        value_rows,
        output_weight,
        expert_ids.T,
        expert_share.T,
        residual,
        norms,
        (gate_weight, up_weight, down_weight),
        (shared_gate, shared_up, shared_down),
    )


def solution(mesh):
    return jax.shard_map(
        local,
        mesh=mesh,
        in_specs=(
            P(("grp", "sp"), "tp"),
            P(("grp", "sp"), "tp"),
            P(("grp", "sp"), "tp"),
            P(("grp", "sp", "tp"), None),
            P("tp", None),
            P(),
            P(),
            P(("grp", "sp", "tp"), None),
            P(("grp", "sp", "tp"), None),
            P(("sp", "tp"), None, None),
            P(("sp", "tp"), None, None),
            P(("sp", "tp"), None, None),
            P(),
            P(),
            P(),
            P(),
            P(),
        ),
        out_specs=P(("grp", "sp", "tp"), None),
        check_vma=False,
    )
```
